32 devices in a mesh: grp: 2 (over y), sp: 4 (over z), tp: 4 (over x, core).
Axes of the slice: x: 2, y: 2, z: 4, core: 2. Of those that a mesh axis runs over, the one named last changes fastest.
Arguments:
- latents: bfloat16 [4096, 2048], P(('grp', 'sp', 'tp')), parts along dimension 0, may hold values from -6 to 6
- conv_value: bfloat16 [4096, 1024], P(('grp', 'sp'), 'tp'), parts along dimension 0, may hold values from -6 to 6
- conv_gate: bfloat16 [4096, 1024], P(('grp', 'sp'), 'tp'), parts along dimension 0, may hold values from -6 to 6
- conv_taps: float32 [31, 1024], P(None, 'tp'), may hold values from -2.2 to 2.2
- conv_gain: float32 [1024], P('tp'), may hold values from 0.1 to 1.9
- point_weight: bfloat16 [1024, 2048], P('tp'), may hold values from -0.1875 to 0.1875
- channel_gain: float32 [2048], replicated, may hold values from 0.1 to 1.9
- expert_ids: int32 [4096, 2], P(('grp', 'sp', 'tp')), parts along dimension 0, may hold values from 0 to 15, all different within a row; in each aligned block of 128 rows (0 to 127, 128 to 255, ...) at most 32 rows name the same one
- expert_weights: float32 [4096, 2], P(('grp', 'sp', 'tp')), parts along dimension 0, may hold values from 0.2 to 1
- gate_weight: bfloat16 [16, 2048, 768], P(('sp', 'tp')), may hold values from -0.125 to 0.125
- up_weight: bfloat16 [16, 2048, 768], P(('sp', 'tp')), may hold values from -0.125 to 0.125
- down_weight: bfloat16 [16, 768, 2048], P(('sp', 'tp')), may hold values from -0.21875 to 0.21875
Outputs:
- result: bfloat16 [4096, 2048], P(('grp', 'sp', 'tp')), parts along dimension 0
The draws below stay inside these ranges and needn't reach their ends.
There are 2 independent parts, one for each index of `grp`. The reference program is written for one: setup_inputs(seed, part) draws one part's arguments, and reference() takes and returns one part's arrays. A program takes and returns all parts, laid end to end along the dimension named above; an argument that names none is the same for every part. Nothing has to cross between parts.
Inputs may be any that keep to these rules, and one draw needn't show every extreme that they name: `expert_ids`: each row names 2 different experts. Within the rows of one device (aligned blocks of 128 rows) no expert is named by more than 32 rows, and in some device's rows some expert is named by exactly 32.
All inputs are finite; a program needn't handle non-finite values.
Results may differ from the reference program's by a relative error of at most 0.012.
Values may be sent and summed in bfloat16 or wider, within the bound.
A program may use at most 64 MiB of HBM per device.

```python
import math
import jax
import jax.numpy as jnp
import numpy as np
from jax import lax

D = 2048
CONV_WIDTH = 1024
KERNEL = 31
EXPERT_WIDTH = 768
TOP_K = 2
TOK_DEV = 128
EXPERTS = 16
TOKENS = 2048
CAP = 32


def draw_conv_taps(key, part):
    first_key, second_key = jax.random.split(jax.random.fold_in(key, 11))
    base = jax.random.truncated_normal(first_key, -3.0, 3.0, (KERNEL, CONV_WIDTH), jnp.float32)
    block_logs = jax.random.uniform(second_key, (16,), jnp.float32, -1.38, 1.38)
    channel_scale = jnp.repeat(jnp.exp(block_logs), CONV_WIDTH // 16)
    return base * KERNEL ** (-0.5) * channel_scale[None, :]


def block_scale(key, shape, cuts, least, top_value):
    level = 1.0
    for position, parts in cuts:
        steps = jax.random.uniform(jax.random.fold_in(jax.random.fold_in(key, 6), position), (parts,), jnp.float32, least / len(cuts), top_value / len(cuts))
        level = level * jnp.repeat(jnp.exp(steps), shape[position] // parts).reshape((-1,) + (1,) * (len(shape) - 1 - position))
    return level


def deal_out(own_key, own, number, rows, number_of, top, bound, skew):
    sequence = jax.random.permutation(own_key, number_of)
    heavy_load, ordinary = portions_of(number_of, rows * top, bound, skew, True), portions_of(number_of, rows * top, bound, skew, False)
    places = jnp.arange(number_of)

    def named(tallies, rotation):
        used = int((tallies > 0).sum())
        fixed = max(1, used // 4)
        passed = fixed + (places - fixed + rotation * (used - fixed)) % max(1, number_of - fixed)
        return jnp.zeros((number_of,), jnp.int32).at[sequence[jnp.where(places < fixed, places, passed)]].set(jnp.asarray(tallies, jnp.int32))

    tallies = jnp.where(number % 4 == 0, named(heavy_load, number // 4), named(ordinary, number - number // 4 - 1))
    mixed = jax.random.permutation(jax.random.fold_in(own, 3), number_of)
    source_of, receiver = mixed[0:number_of // 2 * 2:2], mixed[1:number_of // 2 * 2:2]
    margin = jnp.minimum(tallies[source_of] - 1, bound - tallies[receiver]) // 2
    margin = jnp.where((source_of == sequence[0]) | (receiver == sequence[0]) | (tallies[receiver] == 0), 0, jnp.maximum(margin, 0))
    passed = jax.random.randint(jax.random.fold_in(own, 4), (number_of // 2,), 0, 1 << 20) % (margin + 1)
    tallies = tallies.at[source_of].add(-passed).at[receiver].add(passed)
    labels = jnp.searchsorted(jnp.cumsum(tallies), jnp.arange(rows * top), side="right").astype(jnp.int32)
    grid = labels.reshape(top, rows).T
    grid = grid[jax.random.permutation(jax.random.fold_in(own, 1), rows)]
    rotation = jax.random.randint(jax.random.fold_in(own, 2), (rows, 1), 0, top)
    return jnp.take_along_axis(grid, (jnp.arange(top)[None, :] + rotation) % top, axis=1)


def portions_of(amount, total, bound, slope, full):
    weights = [(1 << 20) // math.isqrt(grade ** slope) + 1 for grade in range(1, amount + 1)]
    largest = bound if full else min(bound, max(-(-total // amount), total * weights[0] // sum(weights)))
    least = 1 if total - largest >= amount - 1 else 0
    holding, rest = [largest] + [least] * (amount - 1), total - largest - least * (amount - 1)
    while rest > 0:
        free = [i for i in range(1, amount) if holding[i] < largest] or [i for i in range(1, amount) if holding[i] < bound]
        pool, remaining = sum([weights[i] for i in free]), rest
        for i in free:
            more = min(bound - holding[i], max(1, remaining * weights[i] // pool), rest)
            holding[i] = holding[i] + more
            rest = rest - more
    return np.array(holding)


def bell_draw(rng, extent, width, limit, pieces=(), kind=jnp.bfloat16):
    result = jax.random.normal(rng, extent, jnp.float32) * width
    if len(pieces) > 0:
        result = block_scale(rng, extent, pieces, -0.22, 0.18) * result
    return jnp.clip(result, min=-limit, max=limit).astype(kind)


def setup_inputs(seed: int = 0, part: int = 0) -> dict:
    splits = jax.random.split(jax.random.key(seed), 13)
    part_splits = jax.random.split(jax.random.fold_in(splits[12], part), 13)
    latents = bell_draw(part_splits[0], (TOKENS, D), 1.0, 6.0, ((0, 16),))
    conv_value = bell_draw(part_splits[1], (TOKENS, CONV_WIDTH), 1.0, 6.0, ((0, 4), (1, 4)))
    conv_gate = bell_draw(part_splits[2], (TOKENS, CONV_WIDTH), 1.0, 6.0, ((0, 4), (1, 4)))
    conv_taps = draw_conv_taps(jax.random.fold_in(splits[12], 71), part)
    conv_gain = jnp.clip(1.0 + 0.18 * jax.random.normal(splits[4], (CONV_WIDTH,), jnp.float32), 0.1, 1.9)
    point_weight = bell_draw(splits[5], (CONV_WIDTH, D), CONV_WIDTH ** -0.5, 0.1875, ((0, 4),))
    channel_gain = jnp.clip(1.0 + 0.18 * jax.random.normal(splits[6], (D,), jnp.float32), 0.1, 1.9)
    expert_ids_keys = jax.random.split(jax.random.fold_in(part_splits[7], 1), TOKENS // TOK_DEV)
    expert_ids_turns = jax.random.permutation(jax.random.fold_in(part_splits[7], 3), TOKENS // TOK_DEV)
    expert_ids = jax.vmap(lambda own, number: deal_out(jax.random.fold_in(part_splits[7], 2), own, number, TOK_DEV, EXPERTS, TOP_K, CAP, 2))(expert_ids_keys, expert_ids_turns).reshape((TOKENS, TOP_K))
    expert_weights = jnp.clip(0.2 + 0.8 * jax.random.uniform(part_splits[8], (TOKENS, TOP_K), jnp.float32) ** block_scale(part_splits[8], (TOKENS, TOP_K), ((0, 16),), -0.2, 0.2), 0.2, 1.0)
    gate_weight = bell_draw(splits[9], (EXPERTS, D, EXPERT_WIDTH), D ** -0.5, 0.125, ((0, 16),))
    up_weight = bell_draw(splits[10], (EXPERTS, D, EXPERT_WIDTH), D ** -0.5, 0.125, ((0, 16),))
    down_weight = bell_draw(splits[11], (EXPERTS, EXPERT_WIDTH, D), EXPERT_WIDTH ** -0.5, 0.21875, ((0, 16),))
    return dict(latents=latents, conv_value=conv_value, conv_gate=conv_gate, conv_taps=conv_taps, conv_gain=conv_gain, point_weight=point_weight, channel_gain=channel_gain, expert_ids=expert_ids, expert_weights=expert_weights, gate_weight=gate_weight, up_weight=up_weight, down_weight=down_weight)


def reference(latents, conv_value, conv_gate, conv_taps, conv_gain, point_weight, channel_gain, expert_ids, expert_weights, gate_weight, up_weight, down_weight):
    gated_value = (conv_value.astype(jnp.float32) * jax.nn.sigmoid(conv_gate.astype(jnp.float32))).astype(jnp.bfloat16)
    half_span = KERNEL // 2
    padded = jnp.pad(gated_value.astype(jnp.float32), ((half_span, half_span), (0, 0)))
    tap_values = conv_taps.astype(jnp.float32)
    mixed_rows = jnp.zeros(gated_value.shape, jnp.float32)
    for offset in range(KERNEL):
        mixed_rows = mixed_rows + tap_values[offset][None, :] * padded[offset:offset + TOKENS]
    center = lax.optimization_barrier(jnp.mean(mixed_rows, axis=1, keepdims=True))
    spread = lax.optimization_barrier(jnp.mean(mixed_rows * mixed_rows, axis=1, keepdims=True)) - center * center
    activated = jax.nn.silu((mixed_rows - center) * lax.rsqrt(spread + 0.05) * conv_gain.astype(jnp.float32)).astype(jnp.bfloat16)
    branch = jnp.dot(activated, point_weight, preferred_element_type=jnp.float32)
    after_conv = (latents.astype(jnp.float32) + branch).astype(jnp.bfloat16)
    after_wide = after_conv.astype(jnp.float32)
    scale_rows = lax.rsqrt(lax.optimization_barrier(jnp.mean(after_wide * after_wide, axis=1, keepdims=True)) + 0.01)
    expert_in = (after_wide * scale_rows * channel_gain.astype(jnp.float32)).astype(jnp.bfloat16)
    blocks = TOKENS // TOK_DEV
    expert_slots = blocks * CAP
    flat_ids = expert_ids.astype(jnp.int32).reshape(blocks, TOK_DEV * TOP_K)
    onehot = (flat_ids[:, :, None] == jnp.arange(EXPERTS, dtype=jnp.int32)[None, None, :]).astype(jnp.int32)
    earlier = lax.optimization_barrier(jnp.sum((jnp.cumsum(onehot, axis=1) - onehot) * onehot, axis=2))
    block_index = jnp.arange(blocks, dtype=jnp.int32)[:, None]
    target = (flat_ids * expert_slots + block_index * CAP + earlier).reshape(-1).astype(jnp.int32)
    token_index = jnp.repeat(jnp.arange(TOKENS, dtype=jnp.int32), TOP_K)
    slot_table = jnp.full((EXPERTS * expert_slots,), TOKENS, jnp.int32).at[target].set(token_index)
    slot_table = slot_table.reshape(EXPERTS, expert_slots)
    padded_in = jnp.concatenate([expert_in, jnp.zeros((1, expert_in.shape[1]), jnp.bfloat16)], axis=0)

    def one_expert(operands):
        row_index, gate_rows, up_rows, down_rows = operands
        chosen = padded_in[row_index]
        gate_part = jnp.dot(chosen, gate_rows, preferred_element_type=jnp.float32)
        up_part = jnp.dot(chosen, up_rows, preferred_element_type=jnp.float32)
        hidden = (jax.nn.silu(gate_part) * up_part).astype(jnp.bfloat16)
        return jnp.dot(hidden, down_rows, preferred_element_type=jnp.float32).astype(jnp.bfloat16)
    outputs = lax.map(one_expert, (slot_table, gate_weight, up_weight, down_weight))
    picked = outputs.reshape(EXPERTS * expert_slots, -1)[target].astype(jnp.float32).reshape(TOKENS, TOP_K, -1)
    routed = lax.optimization_barrier(jnp.sum(expert_weights.astype(jnp.float32)[:, :, None] * picked, axis=1))
    return (after_wide + routed).astype(jnp.bfloat16)
```

```python
import functools

import jax
import jax.numpy as jnp
from jax import lax
from jax.experimental import pallas as pl
from jax.experimental.pallas import tpu as pltpu
from jax.sharding import PartitionSpec as P


def with_halo(block, sides, width):
    for axis, dim in sides:
        count = lax.axis_size(axis)
        forward = [(i, i + 1) for i in range(count - 1)]
        backward = [(target, source) for source, target in forward]
        low = lax.ppermute(
            lax.slice_in_dim(block, block.shape[dim] - width, None, axis=dim), axis, forward
        )
        high = lax.ppermute(lax.slice_in_dim(block, 0, width, axis=dim), axis, backward)
        block = jnp.concatenate([low, block, high], axis=dim)
    return block


MESH = pl.DeviceIdType.MESH
CHUNKS = 4


def expert_kernel(
    n, tp, cap, x_hbm, tab_hbm, after_ref, wg_hbm, wu_hbm, wd_hbm, out_ref,
    toks, tabs, comp, arr, back, inc, acc, wg, wu, wd, hid,
    own_sem, w_sem, tok_send, tok_recv, tab_send, tab_recv,
    piece_send, piece_recv, back_send, back_recv, sum_send, sum_recv,
):
    z = lax.axis_index("sp")
    t = lax.axis_index("tp")
    rows, width = after_ref.shape
    slots = tp * cap
    hidden_width = wg.shape[1]
    part_rows = rows // CHUNKS
    own_tok = pltpu.make_async_copy(x_hbm, toks.at[z], own_sem.at[0])
    own_tab = pltpu.make_async_copy(tab_hbm, tabs.at[z], own_sem.at[1])
    own_tok.start()
    own_tab.start()
    loads = [
        pltpu.make_async_copy(a, b, w_sem.at[i])
        for i, (a, b) in enumerate(((wg_hbm.at[0], wg), (wu_hbm.at[0], wu), (wd_hbm.at[0], wd)))
    ]
    for load in loads:
        load.start()

    barrier = pltpu.get_barrier_semaphore()
    for p in range(1, tp):
        pl.semaphore_signal(
            barrier, inc=1, device_id={"tp": lax.rem(t + p, tp)}, device_id_type=MESH
        )

    @pl.when(z > 0)
    def _():
        pl.semaphore_signal(barrier, inc=1, device_id={"sp": z - 1}, device_id_type=MESH)

    @pl.when(z < n - 1)
    def _():
        pl.semaphore_signal(barrier, inc=1, device_id={"sp": z + 1}, device_id_type=MESH)

    peers = tp - 1 + (z > 0).astype(jnp.int32) + (z < n - 1).astype(jnp.int32)
    pl.semaphore_wait(barrier, peers)

    own_tok.wait()
    own_tab.wait()

    def source(j):
        low = jnp.minimum(z, n - 1 - z)
        near = jnp.where(j % 2 == 1, z - (j + 1) // 2, z + j // 2)
        far = jnp.where(z > n - 1 - z, z - (j - low), z + (j - low))
        return jnp.where(j <= 2 * low, near, far)

    def token_copies(zs, side):
        target = z + 1 if side else z - 1
        return [
            pltpu.make_async_remote_copy(
                src_ref=ref.at[zs],
                dst_ref=ref.at[zs],
                send_sem=ss.at[side, zs],
                recv_sem=rs.at[zs],
                device_id={"sp": target},
                device_id_type=MESH,
            )
            for ref, ss, rs in ((tabs, tab_send, tab_recv), (toks, tok_send, tok_recv))
        ]

    def span(index):
        return pl.ds(pl.multiple_of(index * cap, 16), cap)

    def exchange(j, to_ref, zs, ss, rs):
        page = lax.rem(j, 2)
        for p in range(1, tp):
            other = lax.rem(t + p, tp)
            pltpu.make_async_remote_copy(
                src_ref=comp.at[page, span(other)],
                dst_ref=to_ref.at[zs, span(t)],
                send_sem=ss.at[zs],
                recv_sem=rs.at[zs],
                device_id={"tp": other},
                device_id_type=MESH,
            ).start()
        to_ref[zs, span(t)] = comp[page, span(t)]

    def wait_pieces(ref, zs, ss, rs):
        part = ref.at[zs, pl.ds(0, (tp - 1) * cap)]
        pltpu.make_async_copy(part, part, rs.at[zs]).wait()
        pltpu.make_async_copy(part, part, ss.at[zs]).wait()

    def sum_copy(zs, k, side):
        target = z + 1 if side else z - 1
        slot = jnp.where(target == zs, n, zs) if side else zs
        piece = pl.ds(k * part_rows, part_rows)
        return pltpu.make_async_remote_copy(
            src_ref=toks.at[zs, piece],
            dst_ref=inc.at[slot, piece],
            send_sem=sum_send.at[zs, k],
            recv_sem=sum_recv.at[slot, k],
            device_id={"sp": target},
            device_id_type=MESH,
        )

    def names(zs):
        table = tabs[zs]
        base = (z * slots).astype(jnp.float32)
        place = lax.broadcasted_iota(jnp.int32, (slots, rows), 0).astype(jnp.float32) + base
        return place == table[0:1, :], place == table[1:2, :], table

    def take(j):
        zs = source(j)

        @pl.when(j > 0)
        def _():
            pltpu.make_async_copy(tabs.at[zs], tabs.at[zs], tab_recv.at[zs]).wait()
            pltpu.make_async_copy(toks.at[zs], toks.at[zs], tok_recv.at[zs]).wait()

        @pl.when((zs <= z) & (z < n - 1))
        def _():
            for copy in token_copies(zs, 1):
                copy.start()

        @pl.when((zs >= z) & (z > 0))
        def _():
            for copy in token_copies(zs, 0):
                copy.start()

        first, second, _ = names(zs)
        pick = jnp.where(first | second, 1.0, 0.0).astype(jnp.bfloat16)
        comp[lax.rem(j, 2)] = jnp.dot(pick, toks[zs], preferred_element_type=jnp.float32).astype(jnp.bfloat16)
        exchange(j, arr, zs, piece_send, piece_recv)

    def run(j):
        zs = source(j)

        @pl.when(j == 0)
        def _():
            for load in loads:
                load.wait()

        wait_pieces(arr, zs, piece_send, piece_recv)
        step = 256
        for f in range(0, hidden_width, step):
            gate = jnp.dot(arr[zs], wg[:, f : f + step], preferred_element_type=jnp.float32)
            up = jnp.dot(arr[zs], wu[:, f : f + step], preferred_element_type=jnp.float32)
            hid[:, f : f + step] = (jax.nn.silu(gate) * up).astype(jnp.bfloat16)
        step = 512
        for c in range(0, width, step):
            comp[lax.rem(j, 2), :, c : c + step] = jnp.dot(
                hid[...], wd[:, c : c + step], preferred_element_type=jnp.float32
            ).astype(jnp.bfloat16)
        exchange(j, back, zs, back_send, back_recv)

    def merge(j):
        zs = source(j)
        wait_pieces(back, zs, back_send, back_recv)
        first, second, table = names(zs)
        share = jnp.where(first, table[2:3, :], 0.0) + jnp.where(second, table[3:4, :], 0.0)
        share = share.T
        high = share.astype(jnp.bfloat16)
        rest = (share - high.astype(jnp.float32)).astype(jnp.bfloat16)

        def total():
            return jnp.dot(high, back[zs], preferred_element_type=jnp.float32) + jnp.dot(
                rest, back[zs], preferred_element_type=jnp.float32
            )

        @pl.when((zs <= z) & (z < n - 1))
        def _():
            for copy in token_copies(zs, 1):
                copy.wait_send()

        @pl.when((zs >= z) & (z > 0))
        def _():
            for copy in token_copies(zs, 0):
                copy.wait_send()

        value = total()

        @pl.when(zs == z)
        def _():
            acc[...] = value

        @pl.when(zs != z)
        def _():
            toks[zs] = value.astype(jnp.bfloat16)

        @pl.when((zs < z) & (z == n - 1))
        def _():
            for k in range(CHUNKS):
                sum_copy(zs, k, 0).start()

        @pl.when((zs > z) & (z == 0))
        def _():
            for k in range(CHUNKS):
                sum_copy(zs, k, 1).start()

    def body(j, carry):
        @pl.when(j > 0)
        def _():
            run(j - 1)

        @pl.when(j < n)
        def _():
            take(j)

        @pl.when(j > 0)
        def _():
            merge(j - 1)

        return carry

    lax.fori_loop(0, n + 1, body, 0)

    def relay(side):
        def one(d, carry):
            zs = z + d if side else z - d

            @pl.when((zs <= n - 1) if side else (zs >= 0))
            def _():
                for k in range(CHUNKS):
                    piece = pl.ds(k * part_rows, part_rows)
                    spot = inc.at[zs, piece]
                    pltpu.make_async_copy(spot, spot, sum_recv.at[zs, k]).wait()
                    toks[zs, piece] = (
                        toks[zs, piece].astype(jnp.float32) + inc[zs, piece].astype(jnp.float32)
                    ).astype(jnp.bfloat16)
                    sum_copy(zs, k, side).start()

            return carry

        lax.fori_loop(1, n - 1, one, 0)

    upper = z > n - 1 - z

    @pl.when(upper & (z < n - 1))
    def _():
        relay(0)

    @pl.when(z > 0)
    def _():
        relay(1)

    @pl.when((z <= n - 1 - z) & (z < n - 1))
    def _():
        relay(0)

    for k in range(CHUNKS):
        piece = pl.ds(k * part_rows, part_rows)

        @pl.when(z < n - 1)
        def _():
            spot = inc.at[z, piece]
            pltpu.make_async_copy(spot, spot, sum_recv.at[z, k]).wait()
            acc[piece] = acc[piece] + inc[z, piece].astype(jnp.float32)

        @pl.when(z > 0)
        def _():
            spot = inc.at[n, piece]
            pltpu.make_async_copy(spot, spot, sum_recv.at[n, k]).wait()
            acc[piece] = acc[piece] + inc[n, piece].astype(jnp.float32)

        out_ref[piece] = (after_ref[piece].astype(jnp.float32) + acc[piece]).astype(jnp.bfloat16)

    def drain(zs, carry):
        @pl.when(zs != z)
        def _():
            for k in range(CHUNKS):
                spot = toks.at[zs, pl.ds(k * part_rows, part_rows)]
                pltpu.make_async_copy(spot, spot, sum_send.at[zs, k]).wait()

        return carry

    lax.fori_loop(0, n, drain, 0)


def experts_and_back(expert_in, table, after, gate_weight, up_weight, down_weight, cap):
    n, tp = lax.axis_size("sp"), lax.axis_size("tp")
    rows, width = expert_in.shape
    hidden_width = gate_weight.shape[2]
    slots = tp * cap
    dma = pltpu.SemaphoreType.DMA
    bf16, f32 = jnp.bfloat16, jnp.float32
    anywhere = pl.BlockSpec(memory_space=pl.ANY)
    vmem = pl.BlockSpec(memory_space=pltpu.VMEM)
    return pl.pallas_call(
        functools.partial(expert_kernel, n, tp, cap),
        out_shape=jax.ShapeDtypeStruct((rows, width), bf16),
        in_specs=[anywhere, anywhere, vmem, anywhere, anywhere, anywhere],
        out_specs=vmem,
        scratch_shapes=[
            pltpu.VMEM((n, rows, width), bf16),
            pltpu.VMEM((n,) + table.shape, f32),
            pltpu.VMEM((2, slots, width), bf16),
            pltpu.VMEM((n, slots, width), bf16),
            pltpu.VMEM((n, slots, width), bf16),
            pltpu.VMEM((n + 1, rows, width), bf16),
            pltpu.VMEM((rows, width), f32),
            pltpu.VMEM((width, hidden_width), bf16),
            pltpu.VMEM((width, hidden_width), bf16),
            pltpu.VMEM((hidden_width, width), bf16),
            pltpu.VMEM((slots, hidden_width), bf16),
            dma((2,)),
            dma((3,)),
            dma((2, n)),
            dma((n,)),
            dma((2, n)),
            dma((n,)),
            dma((n,)),
            dma((n,)),
            dma((n,)),
            dma((n,)),
            dma((n, CHUNKS)),
            dma((n + 1, CHUNKS)),
        ],
        compiler_params=pltpu.CompilerParams(
            collective_id=0, has_side_effects=True, vmem_limit_bytes=67043328
        ),
        name="experts",
    )(expert_in, table, after, gate_weight, up_weight, down_weight)


def shards(
    latents,
    conv_value,
    conv_gate,
    conv_taps,
    conv_gain,
    point_weight,
    channel_gain,
    expert_ids,
    expert_weights,
    gate_weight,
    up_weight,
    down_weight,
):
    gated_value = (
        conv_value.astype(jnp.float32) * jax.nn.sigmoid(conv_gate.astype(jnp.float32))
    ).astype(jnp.bfloat16)
    tap_count = conv_taps.shape[0]
    half_span = tap_count // 2
    block_rows = gated_value.shape[0]
    padded = with_halo(gated_value, (("sp", 0),), half_span).astype(jnp.float32)
    mixed_rows = jnp.zeros(gated_value.shape, jnp.float32)
    for offset in range(tap_count):
        mixed_rows = mixed_rows + conv_taps[offset][None, :] * padded[offset : offset + block_rows]
    width_all = conv_value.shape[1] * lax.axis_size("tp")
    sum_values, squares = lax.psum(
        (jnp.sum(mixed_rows, axis=1), jnp.sum(mixed_rows * mixed_rows, axis=1)), "tp"
    )
    center = (sum_values / width_all)[:, None]
    spread = (squares / width_all)[:, None] - center * center
    activated = jax.nn.silu((mixed_rows - center) * lax.rsqrt(spread + 0.05) * conv_gain).astype(
        jnp.bfloat16
    )
    row_count = latents.shape[0]
    by_token = lax.all_to_all(activated, "tp", split_axis=0, concat_axis=1, tiled=True)
    branch = jnp.dot(
        by_token,
        lax.all_gather(point_weight, "tp", axis=0, tiled=True),
        preferred_element_type=jnp.float32,
    )
    after_wide = (latents.astype(jnp.float32) + branch).astype(jnp.bfloat16).astype(jnp.float32)
    scale_rows = lax.rsqrt(jnp.mean(after_wide * after_wide, axis=1, keepdims=True) + 0.01)
    expert_in = (after_wide * scale_rows * channel_gain).astype(jnp.bfloat16)
    local_count = gate_weight.shape[0]
    members = lax.axis_size(("sp", "tp"))
    experts = local_count * members
    top_count = expert_ids.shape[1]
    capacity = 2 * top_count * row_count // experts
    room = -(-capacity // 16) * 16
    flat_ids = expert_ids.reshape(-1)
    onehot = (flat_ids[:, None] == jnp.arange(experts, dtype=jnp.int32)[None, :]).astype(jnp.int32)
    earlier = jnp.sum((jnp.cumsum(onehot, axis=0) - onehot) * onehot, axis=1)
    target = (flat_ids * room + earlier).reshape(row_count, top_count)
    table = jnp.concatenate(
        [
            target.astype(jnp.float32).T,
            expert_weights.T,
            jnp.zeros((8 - 2 * top_count, row_count), jnp.float32),
        ],
        axis=0,
    )
    return experts_and_back(
        expert_in, table, after_wide.astype(jnp.bfloat16), gate_weight, up_weight, down_weight, room
    )


def solution(mesh):
    return jax.shard_map(
        shards,
        mesh=mesh,
        in_specs=(
            P(("grp", "sp", "tp"), None),
            P(("grp", "sp"), "tp"),
            P(("grp", "sp"), "tp"),
            P(None, "tp"),
            P("tp"),
            P("tp", None),
            P(),
            P(("grp", "sp", "tp"), None),
            P(("grp", "sp", "tp"), None),
            P(("sp", "tp"), None, None),
            P(("sp", "tp"), None, None),
            P(("sp", "tp"), None, None),
        ),
        out_specs=P(("grp", "sp", "tp"), None),
        check_vma=False,
    )
```

```python
import functools

import jax
import jax.numpy as jnp
from jax import lax
from jax.experimental import pallas as pl
from jax.experimental.pallas import tpu as pltpu
from jax.sharding import PartitionSpec as P


def with_halo(block, sides, width):
    for axis, dim in sides:
        count = lax.axis_size(axis)
        forward = [(i, i + 1) for i in range(count - 1)]
        backward = [(target, source) for source, target in forward]
        low = lax.ppermute(
            lax.slice_in_dim(block, block.shape[dim] - width, None, axis=dim), axis, forward
        )
        high = lax.ppermute(lax.slice_in_dim(block, 0, width, axis=dim), axis, backward)
        block = jnp.concatenate([low, block, high], axis=dim)
    return block


MESH = pl.DeviceIdType.MESH
CHUNKS = 4


def expert_kernel(
    n, tp, cap, x_hbm, tab_hbm, after_ref, wg_hbm, wu_hbm, wd_hbm, out_ref,
    toks, tabs, comp, arr, back, inc, acc, wg, wu, wd, hid,
    own_sem, w_sem, tok_send, tok_recv, tab_send, tab_recv,
    piece_send, piece_recv, back_send, back_recv, sum_send, sum_recv,
):
    z = lax.axis_index("sp")
    t = lax.axis_index("tp")
    rows, width = after_ref.shape
    slots = tp * cap
    hidden_width = wg.shape[1]
    part_rows = rows // CHUNKS
    own_tok = pltpu.make_async_copy(x_hbm, toks.at[z], own_sem.at[0])
    own_tab = pltpu.make_async_copy(tab_hbm, tabs.at[z], own_sem.at[1])
    own_tok.start()
    own_tab.start()
    loads = [
        pltpu.make_async_copy(a, b, w_sem.at[i])
        for i, (a, b) in enumerate(((wg_hbm.at[0], wg), (wu_hbm.at[0], wu), (wd_hbm.at[0], wd)))
    ]
    for load in loads:
        load.start()

    barrier = pltpu.get_barrier_semaphore()
    for p in range(1, tp):
        pl.semaphore_signal(
            barrier, inc=1, device_id={"tp": lax.rem(t + p, tp)}, device_id_type=MESH
        )

    @pl.when(z > 0)
    def _():
        pl.semaphore_signal(barrier, inc=1, device_id={"sp": z - 1}, device_id_type=MESH)

    @pl.when(z < n - 1)
    def _():
        pl.semaphore_signal(barrier, inc=1, device_id={"sp": z + 1}, device_id_type=MESH)

    peers = tp - 1 + (z > 0).astype(jnp.int32) + (z < n - 1).astype(jnp.int32)
    pl.semaphore_wait(barrier, peers)

    own_tok.wait()
    own_tab.wait()

    def source(j):
        low = jnp.minimum(z, n - 1 - z)
        near = jnp.where(j % 2 == 1, z - (j + 1) // 2, z + j // 2)
        far = jnp.where(z > n - 1 - z, z - (j - low), z + (j - low))
        return jnp.where(j <= 2 * low, near, far)

    def token_copies(zs, side):
        target = z + 1 if side else z - 1
        return [
            pltpu.make_async_remote_copy(
                src_ref=ref.at[zs],
                dst_ref=ref.at[zs],
                send_sem=ss.at[side, zs],
                recv_sem=rs.at[zs],
                device_id={"sp": target},
                device_id_type=MESH,
            )
            for ref, ss, rs in ((tabs, tab_send, tab_recv), (toks, tok_send, tok_recv))
        ]

    def span(index):
        return pl.ds(pl.multiple_of(index * cap, 16), cap)

    def exchange(j, to_ref, zs, ss, rs):
        page = lax.rem(j, 2)
        for p in range(1, tp):
            other = lax.rem(t + p, tp)
            pltpu.make_async_remote_copy(
                src_ref=comp.at[page, span(other)],
                dst_ref=to_ref.at[zs, span(t)],
                send_sem=ss.at[zs],
                recv_sem=rs.at[zs],
                device_id={"tp": other},
                device_id_type=MESH,
            ).start()
        to_ref[zs, span(t)] = comp[page, span(t)]

    def wait_pieces(ref, zs, ss, rs):
        part = ref.at[zs, pl.ds(0, (tp - 1) * cap)]
        pltpu.make_async_copy(part, part, rs.at[zs]).wait()
        pltpu.make_async_copy(part, part, ss.at[zs]).wait()

    def sum_copy(zs, k, side):
        target = z + 1 if side else z - 1
        slot = jnp.where(target == zs, n, zs) if side else zs
        piece = pl.ds(k * part_rows, part_rows)
        return pltpu.make_async_remote_copy(
            src_ref=toks.at[zs, piece],
            dst_ref=inc.at[slot, piece],
            send_sem=sum_send.at[zs, k],
            recv_sem=sum_recv.at[slot, k],
            device_id={"sp": target},
            device_id_type=MESH,
        )

    def names(zs):
        table = tabs[zs]
        base = (z * slots).astype(jnp.float32)
        place = lax.broadcasted_iota(jnp.int32, (slots, rows), 0).astype(jnp.float32) + base
        return place == table[0:1, :], place == table[1:2, :], table

    def passes_on(zs):
        return ((zs <= z) & (z < n - 1)) | ((zs >= z) & (z > 0))

    def arrive(zs):
        pltpu.make_async_copy(tabs.at[zs], tabs.at[zs], tab_recv.at[zs]).wait()
        pltpu.make_async_copy(toks.at[zs], toks.at[zs], tok_recv.at[zs]).wait()

    def forward(zs):
        @pl.when((zs <= z) & (z < n - 1))
        def _():
            for copy in token_copies(zs, 1):
                copy.start()

        @pl.when((zs >= z) & (z > 0))
        def _():
            for copy in token_copies(zs, 0):
                copy.start()

    def hand_on(j):
        zs = source(j)

        @pl.when((j < n) & passes_on(zs))
        def _():
            arrive(zs)
            forward(zs)

    def take(j):
        zs = source(j)

        @pl.when((j > 0) & jnp.logical_not(passes_on(zs)))
        def _():
            arrive(zs)

        first, second, _ = names(zs)
        pick = jnp.where(first | second, 1.0, 0.0).astype(jnp.bfloat16)
        comp[lax.rem(j, 2)] = jnp.dot(pick, toks[zs], preferred_element_type=jnp.float32).astype(jnp.bfloat16)
        exchange(j, arr, zs, piece_send, piece_recv)

    def run(j):
        zs = source(j)

        @pl.when(j == 0)
        def _():
            for load in loads:
                load.wait()

        wait_pieces(arr, zs, piece_send, piece_recv)
        step = 256
        for f in range(0, hidden_width, step):
            gate = jnp.dot(arr[zs], wg[:, f : f + step], preferred_element_type=jnp.float32)
            up = jnp.dot(arr[zs], wu[:, f : f + step], preferred_element_type=jnp.float32)
            hid[:, f : f + step] = (jax.nn.silu(gate) * up).astype(jnp.bfloat16)
        step = 512
        for c in range(0, width, step):
            comp[lax.rem(j, 2), :, c : c + step] = jnp.dot(
                hid[...], wd[:, c : c + step], preferred_element_type=jnp.float32
            ).astype(jnp.bfloat16)
        exchange(j, back, zs, back_send, back_recv)

    def merge(j):
        zs = source(j)
        wait_pieces(back, zs, back_send, back_recv)
        first, second, table = names(zs)
        share = jnp.where(first, table[2:3, :], 0.0) + jnp.where(second, table[3:4, :], 0.0)
        share = share.T
        high = share.astype(jnp.bfloat16)
        rest = (share - high.astype(jnp.float32)).astype(jnp.bfloat16)

        def total():
            return jnp.dot(high, back[zs], preferred_element_type=jnp.float32) + jnp.dot(
                rest, back[zs], preferred_element_type=jnp.float32
            )

        @pl.when((zs <= z) & (z < n - 1))
        def _():
            for copy in token_copies(zs, 1):
                copy.wait_send()

        @pl.when((zs >= z) & (z > 0))
        def _():
            for copy in token_copies(zs, 0):
                copy.wait_send()

        value = total()

        @pl.when(zs == z)
        def _():
            acc[...] = value

        @pl.when(zs != z)
        def _():
            toks[zs] = value.astype(jnp.bfloat16)

        @pl.when((zs < z) & (z == n - 1))
        def _():
            for k in range(CHUNKS):
                sum_copy(zs, k, 0).start()

        @pl.when((zs > z) & (z == 0))
        def _():
            for k in range(CHUNKS):
                sum_copy(zs, k, 1).start()

    forward(z)

    def body(j, carry):
        @pl.when(j > 0)
        def _():
            run(j - 1)

        @pl.when(j == 1)
        def _():
            hand_on(j)

        @pl.when(j > 0)
        def _():
            hand_on(j + 1)

        @pl.when(j < n)
        def _():
            take(j)

        @pl.when(j > 0)
        def _():
            merge(j - 1)

        return carry

    lax.fori_loop(0, n + 1, body, 0)

    def relay(side):
        def one(d, carry):
            zs = z + d if side else z - d

            @pl.when((zs <= n - 1) if side else (zs >= 0))
            def _():
                for k in range(CHUNKS):
                    piece = pl.ds(k * part_rows, part_rows)
                    spot = inc.at[zs, piece]
                    pltpu.make_async_copy(spot, spot, sum_recv.at[zs, k]).wait()
                    toks[zs, piece] = (
                        toks[zs, piece].astype(jnp.float32) + inc[zs, piece].astype(jnp.float32)
                    ).astype(jnp.bfloat16)
                    sum_copy(zs, k, side).start()

            return carry

        lax.fori_loop(1, n - 1, one, 0)

    upper = z > n - 1 - z

    @pl.when(upper & (z < n - 1))
    def _():
        relay(0)

    @pl.when(z > 0)
    def _():
        relay(1)

    @pl.when((z <= n - 1 - z) & (z < n - 1))
    def _():
        relay(0)

    for k in range(CHUNKS):
        piece = pl.ds(k * part_rows, part_rows)

        @pl.when(z < n - 1)
        def _():
            spot = inc.at[z, piece]
            pltpu.make_async_copy(spot, spot, sum_recv.at[z, k]).wait()
            acc[piece] = acc[piece] + inc[z, piece].astype(jnp.float32)

        @pl.when(z > 0)
        def _():
            spot = inc.at[n, piece]
            pltpu.make_async_copy(spot, spot, sum_recv.at[n, k]).wait()
            acc[piece] = acc[piece] + inc[n, piece].astype(jnp.float32)

        out_ref[piece] = (after_ref[piece].astype(jnp.float32) + acc[piece]).astype(jnp.bfloat16)

    def drain(zs, carry):
        @pl.when(zs != z)
        def _():
            for k in range(CHUNKS):
                spot = toks.at[zs, pl.ds(k * part_rows, part_rows)]
                pltpu.make_async_copy(spot, spot, sum_send.at[zs, k]).wait()

        return carry

    lax.fori_loop(0, n, drain, 0)


def experts_and_back(expert_in, table, after, gate_weight, up_weight, down_weight, cap):
    n, tp = lax.axis_size("sp"), lax.axis_size("tp")
    rows, width = expert_in.shape
    hidden_width = gate_weight.shape[2]
    slots = tp * cap
    dma = pltpu.SemaphoreType.DMA
    bf16, f32 = jnp.bfloat16, jnp.float32
    anywhere = pl.BlockSpec(memory_space=pl.ANY)
    vmem = pl.BlockSpec(memory_space=pltpu.VMEM)
    return pl.pallas_call(
        functools.partial(expert_kernel, n, tp, cap),
        out_shape=jax.ShapeDtypeStruct((rows, width), bf16),
        in_specs=[anywhere, anywhere, vmem, anywhere, anywhere, anywhere],
        out_specs=vmem,
        scratch_shapes=[
            pltpu.VMEM((n, rows, width), bf16),
            pltpu.VMEM((n,) + table.shape, f32),
            pltpu.VMEM((2, slots, width), bf16),
            pltpu.VMEM((n, slots, width), bf16),
            pltpu.VMEM((n, slots, width), bf16),
            pltpu.VMEM((n + 1, rows, width), bf16),
            pltpu.VMEM((rows, width), f32),
            pltpu.VMEM((width, hidden_width), bf16),
            pltpu.VMEM((width, hidden_width), bf16),
            pltpu.VMEM((hidden_width, width), bf16),
            pltpu.VMEM((slots, hidden_width), bf16),
            dma((2,)),
            dma((3,)),
            dma((2, n)),
            dma((n,)),
            dma((2, n)),
            dma((n,)),
            dma((n,)),
            dma((n,)),
            dma((n,)),
            dma((n,)),
            dma((n, CHUNKS)),
            dma((n + 1, CHUNKS)),
        ],
        compiler_params=pltpu.CompilerParams(
            collective_id=0, has_side_effects=True, vmem_limit_bytes=67043328
        ),
        name="experts",
    )(expert_in, table, after, gate_weight, up_weight, down_weight)


def shards(
    latents,
    conv_value,
    conv_gate,
    conv_taps,
    conv_gain,
    point_weight,
    channel_gain,
    expert_ids,
    expert_weights,
    gate_weight,
    up_weight,
    down_weight,
):
    gated_value = (
        conv_value.astype(jnp.float32) * jax.nn.sigmoid(conv_gate.astype(jnp.float32))
    ).astype(jnp.bfloat16)
    tap_count = conv_taps.shape[0]
    half_span = tap_count // 2
    block_rows = gated_value.shape[0]
    padded = with_halo(gated_value, (("sp", 0),), half_span).astype(jnp.float32)
    mixed_rows = jnp.zeros(gated_value.shape, jnp.float32)
    for offset in range(tap_count):
        mixed_rows = mixed_rows + conv_taps[offset][None, :] * padded[offset : offset + block_rows]
    width_all = conv_value.shape[1] * lax.axis_size("tp")
    sum_values, squares = lax.psum(
        (jnp.sum(mixed_rows, axis=1), jnp.sum(mixed_rows * mixed_rows, axis=1)), "tp"
    )
    center = (sum_values / width_all)[:, None]
    spread = (squares / width_all)[:, None] - center * center
    activated = jax.nn.silu((mixed_rows - center) * lax.rsqrt(spread + 0.05) * conv_gain).astype(
        jnp.bfloat16
    )
    row_count = latents.shape[0]
    by_token = lax.all_to_all(activated, "tp", split_axis=0, concat_axis=1, tiled=True)
    branch = jnp.dot(
        by_token,
        lax.all_gather(point_weight, "tp", axis=0, tiled=True),
        preferred_element_type=jnp.float32,
    )
    after_wide = (latents.astype(jnp.float32) + branch).astype(jnp.bfloat16).astype(jnp.float32)
    scale_rows = lax.rsqrt(jnp.mean(after_wide * after_wide, axis=1, keepdims=True) + 0.01)
    expert_in = (after_wide * scale_rows * channel_gain).astype(jnp.bfloat16)
    local_count = gate_weight.shape[0]
    members = lax.axis_size(("sp", "tp"))
    experts = local_count * members
    top_count = expert_ids.shape[1]
    capacity = 2 * top_count * row_count // experts
    room = -(-capacity // 16) * 16
    flat_ids = expert_ids.reshape(-1)
    onehot = (flat_ids[:, None] == jnp.arange(experts, dtype=jnp.int32)[None, :]).astype(jnp.int32)
    earlier = jnp.sum((jnp.cumsum(onehot, axis=0) - onehot) * onehot, axis=1)
    target = (flat_ids * room + earlier).reshape(row_count, top_count)
    table = jnp.concatenate(
        [
            target.astype(jnp.float32).T,
            expert_weights.T,
            jnp.zeros((8 - 2 * top_count, row_count), jnp.float32),
        ],
        axis=0,
    )
    return experts_and_back(
        expert_in, table, after_wide.astype(jnp.bfloat16), gate_weight, up_weight, down_weight, room
    )


def solution(mesh):
    return jax.shard_map(
        shards,
        mesh=mesh,
        in_specs=(
            P(("grp", "sp", "tp"), None),
            P(("grp", "sp"), "tp"),
            P(("grp", "sp"), "tp"),
            P(None, "tp"),
            P("tp"),
            P("tp", None),
            P(),
            P(("grp", "sp", "tp"), None),
            P(("grp", "sp", "tp"), None),
            P(("sp", "tp"), None, None),
            P(("sp", "tp"), None, None),
            P(("sp", "tp"), None, None),
        ),
        out_specs=P(("grp", "sp", "tp"), None),
        check_vma=False,
    )
```

```python
import functools

import jax
import jax.numpy as jnp
from jax import lax
from jax.experimental import pallas as pl
from jax.experimental.pallas import tpu as pltpu
from jax.sharding import PartitionSpec as P


MESH = pl.DeviceIdType.MESH
CHUNKS = 4


def expert_kernel(
    n, tp, cap, x_hbm, tab_hbm, after_ref, wg_hbm, wu_hbm, wd_hbm, out_ref,
    toks, tabs, comp, arr, back, inc, acc, wg, wu, wd, hid,
    own_sem, w_sem, tok_send, tok_recv, tab_send, tab_recv,
    piece_send, piece_recv, back_send, back_recv, sum_send, sum_recv,
):
    z = lax.axis_index("sp")
    t = lax.axis_index("tp")
    rows, width = after_ref.shape
    slots = tp * cap
    hidden_width = wg.shape[1]
    part_rows = rows // CHUNKS
    own_tok = pltpu.make_async_copy(x_hbm, toks.at[z], own_sem.at[0])
    own_tab = pltpu.make_async_copy(tab_hbm, tabs.at[z], own_sem.at[1])
    own_tok.start()
    own_tab.start()
    loads = [
        pltpu.make_async_copy(a, b, w_sem.at[i])
        for i, (a, b) in enumerate(((wg_hbm.at[0], wg), (wu_hbm.at[0], wu), (wd_hbm.at[0], wd)))
    ]
    for load in loads:
        load.start()

    barrier = pltpu.get_barrier_semaphore()
    for p in range(1, tp):
        pl.semaphore_signal(
            barrier, inc=1, device_id={"tp": lax.rem(t + p, tp)}, device_id_type=MESH
        )

    @pl.when(z > 0)
    def _():
        pl.semaphore_signal(barrier, inc=1, device_id={"sp": z - 1}, device_id_type=MESH)

    @pl.when(z < n - 1)
    def _():
        pl.semaphore_signal(barrier, inc=1, device_id={"sp": z + 1}, device_id_type=MESH)

    peers = tp - 1 + (z > 0).astype(jnp.int32) + (z < n - 1).astype(jnp.int32)
    pl.semaphore_wait(barrier, peers)

    own_tok.wait()
    own_tab.wait()

    def source(j):
        low = jnp.minimum(z, n - 1 - z)
        near = jnp.where(j % 2 == 1, z - (j + 1) // 2, z + j // 2)
        far = jnp.where(z > n - 1 - z, z - (j - low), z + (j - low))
        return jnp.where(j <= 2 * low, near, far)

    def token_copies(zs, side):
        target = z + 1 if side else z - 1
        return [
            pltpu.make_async_remote_copy(
                src_ref=ref.at[zs],
                dst_ref=ref.at[zs],
                send_sem=ss.at[side, zs],
                recv_sem=rs.at[zs],
                device_id={"sp": target},
                device_id_type=MESH,
            )
            for ref, ss, rs in ((tabs, tab_send, tab_recv), (toks, tok_send, tok_recv))
        ]

    def span(index):
        return pl.ds(pl.multiple_of(index * cap, 16), cap)

    def exchange(j, to_ref, zs, ss, rs):
        page = lax.rem(j, 2)
        for p in range(1, tp):
            other = lax.rem(t + p, tp)
            pltpu.make_async_remote_copy(
                src_ref=comp.at[page, span(other)],
                dst_ref=to_ref.at[zs, span(t)],
                send_sem=ss.at[zs],
                recv_sem=rs.at[zs],
                device_id={"tp": other},
                device_id_type=MESH,
            ).start()
        to_ref[zs, span(t)] = comp[page, span(t)]

    def wait_pieces(ref, zs, ss, rs):
        part = ref.at[zs, pl.ds(0, (tp - 1) * cap)]
        pltpu.make_async_copy(part, part, rs.at[zs]).wait()
        pltpu.make_async_copy(part, part, ss.at[zs]).wait()

    def sum_copy(zs, k, side):
        target = z + 1 if side else z - 1
        slot = jnp.where(target == zs, n, zs) if side else zs
        piece = pl.ds(k * part_rows, part_rows)
        return pltpu.make_async_remote_copy(
            src_ref=toks.at[zs, piece],
            dst_ref=inc.at[slot, piece],
            send_sem=sum_send.at[zs, k],
            recv_sem=sum_recv.at[slot, k],
            device_id={"sp": target},
            device_id_type=MESH,
        )

    def names(zs):
        table = tabs[zs]
        base = (z * slots).astype(jnp.float32)
        place = lax.broadcasted_iota(jnp.int32, (slots, rows), 0).astype(jnp.float32) + base
        return place == table[0:1, :], place == table[1:2, :], table

    def passes_on(zs):
        return ((zs <= z) & (z < n - 1)) | ((zs >= z) & (z > 0))

    def arrive(zs):
        pltpu.make_async_copy(tabs.at[zs], tabs.at[zs], tab_recv.at[zs]).wait()
        pltpu.make_async_copy(toks.at[zs], toks.at[zs], tok_recv.at[zs]).wait()

    def forward(zs):
        @pl.when((zs <= z) & (z < n - 1))
        def _():
            for copy in token_copies(zs, 1):
                copy.start()

        @pl.when((zs >= z) & (z > 0))
        def _():
            for copy in token_copies(zs, 0):
                copy.start()

    def hand_on(j):
        zs = source(j)

        @pl.when((j < n) & passes_on(zs))
        def _():
            arrive(zs)
            forward(zs)

    def take(j):
        zs = source(j)

        @pl.when((j > 0) & jnp.logical_not(passes_on(zs)))
        def _():
            arrive(zs)

        first, second, _ = names(zs)
        pick = jnp.where(first | second, 1.0, 0.0).astype(jnp.bfloat16)
        comp[lax.rem(j, 2)] = jnp.dot(pick, toks[zs], preferred_element_type=jnp.float32).astype(jnp.bfloat16)
        exchange(j, arr, zs, piece_send, piece_recv)

    def run(j):
        zs = source(j)

        @pl.when(j == 0)
        def _():
            for load in loads:
                load.wait()

        wait_pieces(arr, zs, piece_send, piece_recv)
        step = 256
        for f in range(0, hidden_width, step):
            gate = jnp.dot(arr[zs], wg[:, f : f + step], preferred_element_type=jnp.float32)
            up = jnp.dot(arr[zs], wu[:, f : f + step], preferred_element_type=jnp.float32)
            hid[:, f : f + step] = (jax.nn.silu(gate) * up).astype(jnp.bfloat16)
        step = 512
        for c in range(0, width, step):
            comp[lax.rem(j, 2), :, c : c + step] = jnp.dot(
                hid[...], wd[:, c : c + step], preferred_element_type=jnp.float32
            ).astype(jnp.bfloat16)
        exchange(j, back, zs, back_send, back_recv)

    def merge(j):
        zs = source(j)
        wait_pieces(back, zs, back_send, back_recv)
        first, second, table = names(zs)
        share = jnp.where(first, table[2:3, :], 0.0) + jnp.where(second, table[3:4, :], 0.0)
        share = share.T
        high = share.astype(jnp.bfloat16)
        rest = (share - high.astype(jnp.float32)).astype(jnp.bfloat16)

        def total():
            return jnp.dot(high, back[zs], preferred_element_type=jnp.float32) + jnp.dot(
                rest, back[zs], preferred_element_type=jnp.float32
            )

        @pl.when((zs <= z) & (z < n - 1))
        def _():
            for copy in token_copies(zs, 1):
                copy.wait_send()

        @pl.when((zs >= z) & (z > 0))
        def _():
            for copy in token_copies(zs, 0):
                copy.wait_send()

        value = total()

        @pl.when(zs == z)
        def _():
            acc[...] = value

        @pl.when(zs != z)
        def _():
            toks[zs] = value.astype(jnp.bfloat16)

        @pl.when((zs < z) & (z == n - 1))
        def _():
            for k in range(CHUNKS):
                sum_copy(zs, k, 0).start()

        @pl.when((zs > z) & (z == 0))
        def _():
            for k in range(CHUNKS):
                sum_copy(zs, k, 1).start()

    forward(z)

    def body(j, carry):
        @pl.when(j > 0)
        def _():
            run(j - 1)

        @pl.when(j == 1)
        def _():
            hand_on(j)

        @pl.when(j > 0)
        def _():
            hand_on(j + 1)

        @pl.when(j < n)
        def _():
            take(j)

        @pl.when(j > 0)
        def _():
            merge(j - 1)

        return carry

    lax.fori_loop(0, n + 1, body, 0)

    def relay(side):
        def one(d, carry):
            zs = z + d if side else z - d

            @pl.when((zs <= n - 1) if side else (zs >= 0))
            def _():
                for k in range(CHUNKS):
                    piece = pl.ds(k * part_rows, part_rows)
                    spot = inc.at[zs, piece]
                    pltpu.make_async_copy(spot, spot, sum_recv.at[zs, k]).wait()
                    toks[zs, piece] = (
                        toks[zs, piece].astype(jnp.float32) + inc[zs, piece].astype(jnp.float32)
                    ).astype(jnp.bfloat16)
                    sum_copy(zs, k, side).start()

            return carry

        lax.fori_loop(1, n - 1, one, 0)

    upper = z > n - 1 - z

    @pl.when(upper & (z < n - 1))
    def _():
        relay(0)

    @pl.when(z > 0)
    def _():
        relay(1)

    @pl.when((z <= n - 1 - z) & (z < n - 1))
    def _():
        relay(0)

    for k in range(CHUNKS):
        piece = pl.ds(k * part_rows, part_rows)

        @pl.when(z < n - 1)
        def _():
            spot = inc.at[z, piece]
            pltpu.make_async_copy(spot, spot, sum_recv.at[z, k]).wait()
            acc[piece] = acc[piece] + inc[z, piece].astype(jnp.float32)

        @pl.when(z > 0)
        def _():
            spot = inc.at[n, piece]
            pltpu.make_async_copy(spot, spot, sum_recv.at[n, k]).wait()
            acc[piece] = acc[piece] + inc[n, piece].astype(jnp.float32)

        out_ref[piece] = (after_ref[piece].astype(jnp.float32) + acc[piece]).astype(jnp.bfloat16)

    def drain(zs, carry):
        @pl.when(zs != z)
        def _():
            for k in range(CHUNKS):
                spot = toks.at[zs, pl.ds(k * part_rows, part_rows)]
                pltpu.make_async_copy(spot, spot, sum_send.at[zs, k]).wait()

        return carry

    lax.fori_loop(0, n, drain, 0)


def experts_and_back(expert_in, table, after, gate_weight, up_weight, down_weight, cap):
    n, tp = lax.axis_size("sp"), lax.axis_size("tp")
    rows, width = expert_in.shape
    hidden_width = gate_weight.shape[2]
    slots = tp * cap
    dma = pltpu.SemaphoreType.DMA
    bf16, f32 = jnp.bfloat16, jnp.float32
    anywhere = pl.BlockSpec(memory_space=pl.ANY)
    vmem = pl.BlockSpec(memory_space=pltpu.VMEM)
    return pl.pallas_call(
        functools.partial(expert_kernel, n, tp, cap),
        out_shape=jax.ShapeDtypeStruct((rows, width), bf16),
        in_specs=[anywhere, anywhere, vmem, anywhere, anywhere, anywhere],
        out_specs=vmem,
        scratch_shapes=[
            pltpu.VMEM((n, rows, width), bf16),
            pltpu.VMEM((n,) + table.shape, f32),
            pltpu.VMEM((2, slots, width), bf16),
            pltpu.VMEM((n, slots, width), bf16),
            pltpu.VMEM((n, slots, width), bf16),
            pltpu.VMEM((n + 1, rows, width), bf16),
            pltpu.VMEM((rows, width), f32),
            pltpu.VMEM((width, hidden_width), bf16),
            pltpu.VMEM((width, hidden_width), bf16),
            pltpu.VMEM((hidden_width, width), bf16),
            pltpu.VMEM((slots, hidden_width), bf16),
            dma((2,)),
            dma((3,)),
            dma((2, n)),
            dma((n,)),
            dma((2, n)),
            dma((n,)),
            dma((n,)),
            dma((n,)),
            dma((n,)),
            dma((n,)),
            dma((n, CHUNKS)),
            dma((n + 1, CHUNKS)),
        ],
        compiler_params=pltpu.CompilerParams(
            collective_id=0, has_side_effects=True, vmem_limit_bytes=67043328
        ),
        name="experts",
    )(expert_in, table, after, gate_weight, up_weight, down_weight)


def branch_kernel(
    n, tp, taps_count, value_ref, gate_ref, taps_ref, weight_ref, latent_ref, gain_ref,
    after_ref, in_ref,
    gated, win, low, high, taps, wide, mixed, act, weights, total,
    win_send, win_recv, halo_send, halo_recv, tap_send, tap_recv, w_send, w_pass, w_recv,
):
    z = lax.axis_index("sp")
    t = lax.axis_index("tp")
    block, chans = value_ref.shape
    rows, width = latent_ref.shape
    edge = low.shape[1]
    half = taps_count // 2
    view = rows + 2 * edge
    mate = t + 1 - 2 * lax.rem(t, 2)
    halves = chans // 2

    barrier = pltpu.get_barrier_semaphore()
    for p in range(tp):
        other = lax.rem(t + p, tp)
        if p:
            pl.semaphore_signal(barrier, inc=1, device_id={"tp": other}, device_id_type=MESH)

        @pl.when(z > 0)
        def _():
            pl.semaphore_signal(
                barrier, inc=1, device_id={"sp": z - 1, "tp": other}, device_id_type=MESH
            )

        @pl.when(z < n - 1)
        def _():
            pl.semaphore_signal(
                barrier, inc=1, device_id={"sp": z + 1, "tp": other}, device_id_type=MESH
            )

    gated[pl.ds(0, edge)] = jnp.zeros((edge, chans), jnp.bfloat16)
    gated[pl.ds(edge + block, edge)] = jnp.zeros((edge, chans), jnp.bfloat16)
    step = 64
    for r in range(0, block, step):
        value = value_ref[pl.ds(r, step)].astype(jnp.float32)
        gate = gate_ref[pl.ds(r, step)].astype(jnp.float32)
        gated[pl.ds(edge + r, step)] = (value * jax.nn.sigmoid(gate)).astype(jnp.bfloat16)

    peers = tp - 1 + tp * ((z > 0).astype(jnp.int32) + (z < n - 1).astype(jnp.int32))
    pl.semaphore_wait(barrier, peers)

    def span(index):
        return pl.ds(pl.multiple_of(index * rows, 16), view)

    def win_copy(p):
        other = lax.rem(t + p, tp)
        return pltpu.make_async_remote_copy(
            src_ref=gated.at[span(other)], dst_ref=win.at[t],
            send_sem=win_send.at[p], recv_sem=win_recv.at[t],
            device_id={"tp": other}, device_id_type=MESH,
        )

    def tap_copy(p):
        other = lax.rem(t + p, tp)
        return pltpu.make_async_remote_copy(
            src_ref=taps_ref, dst_ref=taps.at[t],
            send_sem=tap_send.at[p], recv_sem=tap_recv.at[t],
            device_id={"tp": other}, device_id_type=MESH,
        )

    def halo_copy(up):
        start = block if up else edge
        place = low if up else high
        return pltpu.make_async_remote_copy(
            src_ref=gated.at[pl.ds(start, edge)], dst_ref=place.at[t],
            send_sem=halo_send.at[up], recv_sem=halo_recv.at[up, t],
            device_id={"sp": z + 1 if up else z - 1, "tp": jnp.int32(0 if up else tp - 1)},
            device_id_type=MESH,
        )

    @pl.when(z < n - 1)
    def _():
        halo_copy(1).start()

    @pl.when(z > 0)
    def _():
        halo_copy(0).start()

    for p in range(1, tp):
        win_copy(p).start()
        tap_copy(p).start()

    def weight_copy(source, part, target, send_sem, first):
        spot = pl.ds(part * halves, halves)
        return pltpu.make_async_remote_copy(
            src_ref=weight_ref.at[spot] if first else weights.at[source, spot],
            dst_ref=weights.at[source, spot],
            send_sem=send_sem, recv_sem=w_recv.at[source, part],
            device_id={"tp": target}, device_id_type=MESH,
        )

    def own_weights():
        copies = []
        for part in range(2):
            for q in range(1, tp // 2):
                copies.append(
                    weight_copy(t, part, lax.rem(t + 2 * q, tp), w_send.at[q, part], True)
                )
            copies.append(weight_copy(t, part, mate, w_send.at[0, part], True))
        return copies

    for copy in own_weights():
        copy.start()

    win[t] = gated[span(t)]
    taps[t] = taps_ref[...]
    weights[t] = weight_ref[...]

    for p in range(1, tp):
        other = lax.rem(t + p, tp)
        pltpu.make_async_copy(win.at[other], win.at[other], win_recv.at[other]).wait()
        pltpu.make_async_copy(taps.at[other], taps.at[other], tap_recv.at[other]).wait()

    @pl.when((t == 0) & (z > 0))
    def _():
        for s in range(tp):
            pltpu.make_async_copy(low.at[s], low.at[s], halo_recv.at[1, s]).wait()
            win[s, pl.ds(0, edge)] = low[s]

    @pl.when((t == tp - 1) & (z < n - 1))
    def _():
        for s in range(tp):
            pltpu.make_async_copy(high.at[s], high.at[s], halo_recv.at[0, s]).wait()
            win[s, pl.ds(edge + rows, edge)] = high[s]

    def convolve(s, carry):
        first, second = carry
        wide[...] = win[s].astype(jnp.float32)
        tile = 64
        sums, squares = [], []
        for r in range(0, rows, tile):
            value = jnp.zeros((tile, chans), jnp.float32)
            for i in range(taps_count):
                value = value + taps[s, pl.ds(i, 1)] * wide[pl.ds(edge - half + i + r, tile)]
            mixed[s, pl.ds(r, tile)] = value
            sums.append(jnp.sum(value, axis=1, keepdims=True))
            squares.append(jnp.sum(value * value, axis=1, keepdims=True))
        return first + jnp.concatenate(sums, axis=0), second + jnp.concatenate(squares, axis=0)

    zero = jnp.zeros((rows, 1), jnp.float32)
    sums, squares = lax.fori_loop(0, tp, convolve, (zero, zero))
    center = sums / (chans * tp)
    spread = squares / (chans * tp) - center * center
    scale = lax.rsqrt(spread + 0.05)

    def activate(s, carry):
        value = (mixed[s] - center) * scale * taps[s, pl.ds(taps_count, 1)]
        act[s] = jax.nn.silu(value).astype(jnp.bfloat16)
        return carry

    lax.fori_loop(0, tp, activate, 0)

    def multiply(source):
        for c in range(0, width, 512):
            spot = pl.ds(c, 512)
            total[:, spot] += jnp.dot(
                act[source], weights[source, :, spot], preferred_element_type=jnp.float32
            )

    def landed(source):
        for part in range(2):
            spot = weights.at[source, pl.ds(part * halves, halves)]
            pltpu.make_async_copy(spot, spot, w_recv.at[source, part]).wait()

    total[...] = latent_ref[...].astype(jnp.float32)
    multiply(t)
    landed(mate)
    multiply(mate)

    def passing(q, part):
        source = lax.rem(t + 2 * q, tp)
        return weight_copy(source, part, mate, w_pass.at[q, part], False)

    for q in range(1, tp // 2):
        source = lax.rem(t + 2 * q, tp)
        for part in range(2):
            spot = weights.at[source, pl.ds(part * halves, halves)]
            pltpu.make_async_copy(spot, spot, w_recv.at[source, part]).wait()
            passing(q, part).start()
        multiply(source)
    for q in range(1, tp // 2):
        source = lax.rem(mate + 2 * q, tp)
        landed(source)
        multiply(source)

    for r in range(0, rows, 32):
        spot = pl.ds(r, 32)
        after = total[spot].astype(jnp.bfloat16)
        after_ref[spot] = after
        after = after.astype(jnp.float32)
        norm = lax.rsqrt(jnp.mean(after * after, axis=1, keepdims=True) + 0.01)
        in_ref[spot] = (after * norm * gain_ref[...]).astype(jnp.bfloat16)

    for p in range(1, tp):
        win_copy(p).wait_send()
        tap_copy(p).wait_send()
    for copy in own_weights():
        copy.wait_send()
    for q in range(1, tp // 2):
        for part in range(2):
            passing(q, part).wait_send()

    @pl.when(z < n - 1)
    def _():
        halo_copy(1).wait_send()

    @pl.when(z > 0)
    def _():
        halo_copy(0).wait_send()


def branch_and_norm(value, gate, conv_taps, conv_gain, point_weight, latents, channel_gain):
    n, tp = lax.axis_size("sp"), lax.axis_size("tp")
    block, chans = value.shape
    rows, width = latents.shape
    taps_count = conv_taps.shape[0]
    edge = -(-(taps_count // 2) // 16) * 16
    table = jnp.concatenate([conv_taps, conv_gain[None, :]], axis=0)
    table = jnp.pad(table, ((0, -table.shape[0] % 8), (0, 0)))
    dma = pltpu.SemaphoreType.DMA
    bf16, f32 = jnp.bfloat16, jnp.float32
    vmem = pl.BlockSpec(memory_space=pltpu.VMEM)
    return pl.pallas_call(
        functools.partial(branch_kernel, n, tp, taps_count),
        out_shape=[jax.ShapeDtypeStruct((rows, width), bf16)] * 2,
        in_specs=[vmem] * 6,
        out_specs=[vmem] * 2,
        scratch_shapes=[
            pltpu.VMEM((block + 2 * edge, chans), bf16),
            pltpu.VMEM((tp, rows + 2 * edge, chans), bf16),
            pltpu.VMEM((tp, edge, chans), bf16),
            pltpu.VMEM((tp, edge, chans), bf16),
            pltpu.VMEM((tp,) + table.shape, f32),
            pltpu.VMEM((rows + 2 * edge, chans), f32),
            pltpu.VMEM((tp, rows, chans), f32),
            pltpu.VMEM((tp, rows, chans), bf16),
            pltpu.VMEM((tp, chans, width), bf16),
            pltpu.VMEM((rows, width), f32),
            dma((tp,)),
            dma((tp,)),
            dma((2,)),
            dma((2, tp)),
            dma((tp,)),
            dma((tp,)),
            dma((tp // 2, 2)),
            dma((tp // 2, 2)),
            dma((tp, 2)),
        ],
        compiler_params=pltpu.CompilerParams(
            collective_id=1, has_side_effects=True, vmem_limit_bytes=48 * 2**20
        ),
        name="branch",
    )(value, gate, table, point_weight, latents, channel_gain[None, :])


def shards(
    latents,
    conv_value,
    conv_gate,
    conv_taps,
    conv_gain,
    point_weight,
    channel_gain,
    expert_ids,
    expert_weights,
    gate_weight,
    up_weight,
    down_weight,
):
    after, expert_in = branch_and_norm(
        conv_value, conv_gate, conv_taps, conv_gain, point_weight, latents, channel_gain
    )
    row_count = latents.shape[0]
    local_count = gate_weight.shape[0]
    members = lax.axis_size(("sp", "tp"))
    experts = local_count * members
    top_count = expert_ids.shape[1]
    capacity = 2 * top_count * row_count // experts
    room = -(-capacity // 16) * 16
    flat_ids = expert_ids.reshape(-1)
    onehot = (flat_ids[:, None] == jnp.arange(experts, dtype=jnp.int32)[None, :]).astype(jnp.int32)
    earlier = jnp.sum((jnp.cumsum(onehot, axis=0) - onehot) * onehot, axis=1)
    target = (flat_ids * room + earlier).reshape(row_count, top_count)
    table = jnp.concatenate(
        [
            target.astype(jnp.float32).T,
            expert_weights.T,
            jnp.zeros((8 - 2 * top_count, row_count), jnp.float32),
        ],
        axis=0,
    )
    return experts_and_back(
        expert_in, table, after, gate_weight, up_weight, down_weight, room
    )


def solution(mesh):
    return jax.shard_map(
        shards,
        mesh=mesh,
        in_specs=(
            P(("grp", "sp", "tp"), None),
            P(("grp", "sp"), "tp"),
            P(("grp", "sp"), "tp"),
            P(None, "tp"),
            P("tp"),
            P("tp", None),
            P(),
            P(("grp", "sp", "tp"), None),
            P(("grp", "sp", "tp"), None),
            P(("sp", "tp"), None, None),
            P(("sp", "tp"), None, None),
            P(("sp", "tp"), None, None),
        ),
        out_specs=P(("grp", "sp", "tp"), None),
        check_vma=False,
    )
```

```python
import functools

import jax
import jax.numpy as jnp
from jax import lax
from jax.experimental import pallas as pl
from jax.experimental.pallas import tpu as pltpu
from jax.sharding import PartitionSpec as P


MESH = pl.DeviceIdType.MESH
CHUNKS = 8


def expert_kernel(
    n, tp, cap, x_hbm, tab_hbm, after_ref, wg_hbm, wu_hbm, wd_hbm, out_ref,
    toks, tabs, comp, arr, back, inc, acc, wg, wu, wd, hid,
    own_sem, w_sem, tok_send, tok_recv, tab_send, tab_recv,
    piece_send, piece_recv, back_send, back_recv, sum_send, sum_recv,
):
    z = lax.axis_index("sp")
    t = lax.axis_index("tp")
    rows, width = after_ref.shape
    slots = tp * cap
    hidden_width = wg.shape[1]
    part_rows = rows // CHUNKS
    own_tok = pltpu.make_async_copy(x_hbm, toks.at[z], own_sem.at[0])
    own_tab = pltpu.make_async_copy(tab_hbm, tabs.at[z], own_sem.at[1])
    own_tok.start()
    own_tab.start()
    loads = [
        pltpu.make_async_copy(a, b, w_sem.at[i])
        for i, (a, b) in enumerate(((wg_hbm.at[0], wg), (wu_hbm.at[0], wu), (wd_hbm.at[0], wd)))
    ]
    for load in loads:
        load.start()

    barrier = pltpu.get_barrier_semaphore()
    for p in range(1, tp):
        pl.semaphore_signal(
            barrier, inc=1, device_id={"tp": lax.rem(t + p, tp)}, device_id_type=MESH
        )

    @pl.when(z > 0)
    def _():
        pl.semaphore_signal(barrier, inc=1, device_id={"sp": z - 1}, device_id_type=MESH)

    @pl.when(z < n - 1)
    def _():
        pl.semaphore_signal(barrier, inc=1, device_id={"sp": z + 1}, device_id_type=MESH)

    peers = tp - 1 + (z > 0).astype(jnp.int32) + (z < n - 1).astype(jnp.int32)
    pl.semaphore_wait(barrier, peers)

    own_tok.wait()
    own_tab.wait()

    def source(j):
        low = jnp.minimum(z, n - 1 - z)
        near = jnp.where(j % 2 == 1, z - (j + 1) // 2, z + j // 2)
        far = jnp.where(z > n - 1 - z, z - (j - low), z + (j - low))
        return jnp.where(j <= 2 * low, near, far)

    def token_copies(zs, side):
        target = z + 1 if side else z - 1
        return [
            pltpu.make_async_remote_copy(
                src_ref=ref.at[zs],
                dst_ref=ref.at[zs],
                send_sem=ss.at[side, zs],
                recv_sem=rs.at[zs],
                device_id={"sp": target},
                device_id_type=MESH,
            )
            for ref, ss, rs in ((tabs, tab_send, tab_recv), (toks, tok_send, tok_recv))
        ]

    def span(index):
        return pl.ds(pl.multiple_of(index * cap, 16), cap)

    def exchange(j, to_ref, zs, ss, rs):
        page = lax.rem(j, 2)
        for p in range(1, tp):
            other = lax.rem(t + p, tp)
            pltpu.make_async_remote_copy(
                src_ref=comp.at[page, span(other)],
                dst_ref=to_ref.at[zs, span(t)],
                send_sem=ss.at[zs],
                recv_sem=rs.at[zs],
                device_id={"tp": other},
                device_id_type=MESH,
            ).start()
        to_ref[zs, span(t)] = comp[page, span(t)]

    def wait_pieces(ref, zs, ss, rs):
        part = ref.at[zs, pl.ds(0, (tp - 1) * cap)]
        pltpu.make_async_copy(part, part, rs.at[zs]).wait()
        pltpu.make_async_copy(part, part, ss.at[zs]).wait()

    def sum_copy(zs, k, side):
        target = z + 1 if side else z - 1
        slot = jnp.where(target == zs, n, zs) if side else zs
        piece = pl.ds(k * part_rows, part_rows)
        return pltpu.make_async_remote_copy(
            src_ref=toks.at[zs, piece],
            dst_ref=inc.at[slot, piece],
            send_sem=sum_send.at[zs, k],
            recv_sem=sum_recv.at[slot, k],
            device_id={"sp": target},
            device_id_type=MESH,
        )

    def names(zs):
        table = tabs[zs]
        base = (z * slots).astype(jnp.float32)
        place = lax.broadcasted_iota(jnp.int32, (slots, rows), 0).astype(jnp.float32) + base
        return place == table[0:1, :], place == table[1:2, :], table

    def passes_on(zs):
        return ((zs <= z) & (z < n - 1)) | ((zs >= z) & (z > 0))

    def arrive(zs):
        pltpu.make_async_copy(tabs.at[zs], tabs.at[zs], tab_recv.at[zs]).wait()
        pltpu.make_async_copy(toks.at[zs], toks.at[zs], tok_recv.at[zs]).wait()

    def forward(zs):
        @pl.when((zs <= z) & (z < n - 1))
        def _():
            for copy in token_copies(zs, 1):
                copy.start()

        @pl.when((zs >= z) & (z > 0))
        def _():
            for copy in token_copies(zs, 0):
                copy.start()

    def hand_on(j):
        zs = source(j)

        @pl.when((j < n) & passes_on(zs))
        def _():
            arrive(zs)
            forward(zs)

    def take(j):
        zs = source(j)

        @pl.when((j > 0) & jnp.logical_not(passes_on(zs)))
        def _():
            arrive(zs)

        first, second, _ = names(zs)
        pick = jnp.where(first | second, 1.0, 0.0).astype(jnp.bfloat16)
        comp[lax.rem(j, 2)] = jnp.dot(pick, toks[zs], preferred_element_type=jnp.float32).astype(jnp.bfloat16)
        exchange(j, arr, zs, piece_send, piece_recv)

    def run(j):
        zs = source(j)

        @pl.when(j == 0)
        def _():
            for load in loads:
                load.wait()

        wait_pieces(arr, zs, piece_send, piece_recv)
        step = 256
        for f in range(0, hidden_width, step):
            gate = jnp.dot(arr[zs], wg[:, f : f + step], preferred_element_type=jnp.float32)
            up = jnp.dot(arr[zs], wu[:, f : f + step], preferred_element_type=jnp.float32)
            hid[:, f : f + step] = (jax.nn.silu(gate) * up).astype(jnp.bfloat16)
        step = 512
        for c in range(0, width, step):
            comp[lax.rem(j, 2), :, c : c + step] = jnp.dot(
                hid[...], wd[:, c : c + step], preferred_element_type=jnp.float32
            ).astype(jnp.bfloat16)
        exchange(j, back, zs, back_send, back_recv)

    def merge(j):
        zs = source(j)
        wait_pieces(back, zs, back_send, back_recv)
        first, second, table = names(zs)
        share = jnp.where(first, table[2:3, :], 0.0) + jnp.where(second, table[3:4, :], 0.0)
        share = share.T
        high = share.astype(jnp.bfloat16)
        rest = (share - high.astype(jnp.float32)).astype(jnp.bfloat16)

        def total():
            return jnp.dot(high, back[zs], preferred_element_type=jnp.float32) + jnp.dot(
                rest, back[zs], preferred_element_type=jnp.float32
            )

        @pl.when((zs <= z) & (z < n - 1))
        def _():
            for copy in token_copies(zs, 1):
                copy.wait_send()

        @pl.when((zs >= z) & (z > 0))
        def _():
            for copy in token_copies(zs, 0):
                copy.wait_send()

        value = total()

        @pl.when(zs == z)
        def _():
            acc[...] = value

        @pl.when(zs != z)
        def _():
            toks[zs] = value.astype(jnp.bfloat16)

        @pl.when((zs < z) & (z == n - 1))
        def _():
            for k in range(CHUNKS):
                sum_copy(zs, k, 0).start()

        @pl.when((zs > z) & (z == 0))
        def _():
            for k in range(CHUNKS):
                sum_copy(zs, k, 1).start()

    forward(z)

    def body(j, carry):
        @pl.when(j > 0)
        def _():
            run(j - 1)

        @pl.when(j == 1)
        def _():
            hand_on(j)

        @pl.when(j > 0)
        def _():
            hand_on(j + 1)

        @pl.when(j < n)
        def _():
            take(j)

        @pl.when(j > 0)
        def _():
            merge(j - 1)

        return carry

    lax.fori_loop(0, n + 1, body, 0)

    def relay(side):
        def one(d, carry):
            zs = z + d if side else z - d

            @pl.when((zs <= n - 1) if side else (zs >= 0))
            def _():
                for k in range(CHUNKS):
                    piece = pl.ds(k * part_rows, part_rows)
                    spot = inc.at[zs, piece]
                    pltpu.make_async_copy(spot, spot, sum_recv.at[zs, k]).wait()
                    toks[zs, piece] = (
                        toks[zs, piece].astype(jnp.float32) + inc[zs, piece].astype(jnp.float32)
                    ).astype(jnp.bfloat16)
                    sum_copy(zs, k, side).start()

            return carry

        lax.fori_loop(1, n - 1, one, 0)

    upper = z > n - 1 - z

    @pl.when(upper & (z < n - 1))
    def _():
        relay(0)

    @pl.when(z > 0)
    def _():
        relay(1)

    @pl.when((z <= n - 1 - z) & (z < n - 1))
    def _():
        relay(0)

    for k in range(CHUNKS):
        piece = pl.ds(k * part_rows, part_rows)

        @pl.when(z < n - 1)
        def _():
            spot = inc.at[z, piece]
            pltpu.make_async_copy(spot, spot, sum_recv.at[z, k]).wait()
            acc[piece] = acc[piece] + inc[z, piece].astype(jnp.float32)

        @pl.when(z > 0)
        def _():
            spot = inc.at[n, piece]
            pltpu.make_async_copy(spot, spot, sum_recv.at[n, k]).wait()
            acc[piece] = acc[piece] + inc[n, piece].astype(jnp.float32)

        out_ref[piece] = (after_ref[piece].astype(jnp.float32) + acc[piece]).astype(jnp.bfloat16)

    def drain(zs, carry):
        @pl.when(zs != z)
        def _():
            for k in range(CHUNKS):
                spot = toks.at[zs, pl.ds(k * part_rows, part_rows)]
                pltpu.make_async_copy(spot, spot, sum_send.at[zs, k]).wait()

        return carry

    lax.fori_loop(0, n, drain, 0)


def experts_and_back(expert_in, table, after, gate_weight, up_weight, down_weight, cap):
    n, tp = lax.axis_size("sp"), lax.axis_size("tp")
    rows, width = expert_in.shape
    hidden_width = gate_weight.shape[2]
    slots = tp * cap
    dma = pltpu.SemaphoreType.DMA
    bf16, f32 = jnp.bfloat16, jnp.float32
    anywhere = pl.BlockSpec(memory_space=pl.ANY)
    vmem = pl.BlockSpec(memory_space=pltpu.VMEM)
    return pl.pallas_call(
        functools.partial(expert_kernel, n, tp, cap),
        out_shape=jax.ShapeDtypeStruct((rows, width), bf16),
        in_specs=[anywhere, anywhere, vmem, anywhere, anywhere, anywhere],
        out_specs=vmem,
        scratch_shapes=[
            pltpu.VMEM((n, rows, width), bf16),
            pltpu.VMEM((n,) + table.shape, f32),
            pltpu.VMEM((2, slots, width), bf16),
            pltpu.VMEM((n, slots, width), bf16),
            pltpu.VMEM((n, slots, width), bf16),
            pltpu.VMEM((n + 1, rows, width), bf16),
            pltpu.VMEM((rows, width), f32),
            pltpu.VMEM((width, hidden_width), bf16),
            pltpu.VMEM((width, hidden_width), bf16),
            pltpu.VMEM((hidden_width, width), bf16),
            pltpu.VMEM((slots, hidden_width), bf16),
            dma((2,)),
            dma((3,)),
            dma((2, n)),
            dma((n,)),
            dma((2, n)),
            dma((n,)),
            dma((n,)),
            dma((n,)),
            dma((n,)),
            dma((n,)),
            dma((n, CHUNKS)),
            dma((n + 1, CHUNKS)),
        ],
        compiler_params=pltpu.CompilerParams(
            collective_id=0, has_side_effects=True, vmem_limit_bytes=67043328
        ),
        name="experts",
    )(expert_in, table, after, gate_weight, up_weight, down_weight)


def branch_kernel(
    n, tp, taps_count, room, value_hbm, gate_hbm, taps_ref, weight_hbm, latent_hbm, gain_ref,
    ids_ref, share_ref, after_ref, in_ref, table_ref,
    value_ref, gate_ref, latent_ref, load_sem, gated, win, low, high, taps, wide, mixed, act, weights, total,
    win_send, win_recv, halo_send, halo_recv, tap_send, tap_recv, w_send, w_pass, w_recv,
):
    z = lax.axis_index("sp")
    t = lax.axis_index("tp")
    block, chans = value_ref.shape
    rows, width = latent_ref.shape
    edge = low.shape[1]
    half = taps_count // 2
    view = rows + 2 * edge
    mate = t + 1 - 2 * lax.rem(t, 2)
    halves = chans // 2
    loads = [
        pltpu.make_async_copy(a, b, load_sem.at[i])
        for i, (a, b) in enumerate(
            (
                (value_hbm, value_ref),
                (gate_hbm, gate_ref),
                (weight_hbm, weights.at[t]),
                (latent_hbm, latent_ref),
            )
        )
    ]
    for load in loads:
        load.start()

    barrier = pltpu.get_barrier_semaphore()
    for p in range(tp):
        other = lax.rem(t + p, tp)
        if p:
            pl.semaphore_signal(barrier, inc=1, device_id={"tp": other}, device_id_type=MESH)

        @pl.when(z > 0)
        def _():
            pl.semaphore_signal(
                barrier, inc=1, device_id={"sp": z - 1, "tp": other}, device_id_type=MESH
            )

        @pl.when(z < n - 1)
        def _():
            pl.semaphore_signal(
                barrier, inc=1, device_id={"sp": z + 1, "tp": other}, device_id_type=MESH
            )

    gated[pl.ds(0, edge)] = jnp.zeros((edge, chans), jnp.bfloat16)
    gated[pl.ds(edge + block, edge)] = jnp.zeros((edge, chans), jnp.bfloat16)
    loads[0].wait()
    loads[1].wait()
    step = 64
    for r in range(0, block, step):
        value = value_ref[pl.ds(r, step)].astype(jnp.float32)
        gate = gate_ref[pl.ds(r, step)].astype(jnp.float32)
        gated[pl.ds(edge + r, step)] = (value * jax.nn.sigmoid(gate)).astype(jnp.bfloat16)

    peers = tp - 1 + tp * ((z > 0).astype(jnp.int32) + (z < n - 1).astype(jnp.int32))
    pl.semaphore_wait(barrier, peers)

    def span(index):
        return pl.ds(pl.multiple_of(index * rows, 16), view)

    def win_copy(p):
        other = lax.rem(t + p, tp)
        return pltpu.make_async_remote_copy(
            src_ref=gated.at[span(other)], dst_ref=win.at[t],
            send_sem=win_send.at[p], recv_sem=win_recv.at[t],
            device_id={"tp": other}, device_id_type=MESH,
        )

    def tap_copy(p):
        other = lax.rem(t + p, tp)
        return pltpu.make_async_remote_copy(
            src_ref=taps_ref, dst_ref=taps.at[t],
            send_sem=tap_send.at[p], recv_sem=tap_recv.at[t],
            device_id={"tp": other}, device_id_type=MESH,
        )

    def halo_copy(up):
        start = block if up else edge
        place = low if up else high
        return pltpu.make_async_remote_copy(
            src_ref=gated.at[pl.ds(start, edge)], dst_ref=place.at[t],
            send_sem=halo_send.at[up], recv_sem=halo_recv.at[up, t],
            device_id={"sp": z + 1 if up else z - 1, "tp": jnp.int32(0 if up else tp - 1)},
            device_id_type=MESH,
        )

    @pl.when(z < n - 1)
    def _():
        halo_copy(1).start()

    @pl.when(z > 0)
    def _():
        halo_copy(0).start()

    for p in range(1, tp):
        win_copy(p).start()
        tap_copy(p).start()

    loads[2].wait()

    def weight_copy(source, part, target, send_sem):
        spot = pl.ds(part * halves, halves)
        return pltpu.make_async_remote_copy(
            src_ref=weights.at[source, spot],
            dst_ref=weights.at[source, spot],
            send_sem=send_sem, recv_sem=w_recv.at[source, part],
            device_id={"tp": target}, device_id_type=MESH,
        )

    def own_weights():
        copies = []
        for part in range(2):
            for q in range(1, tp // 2):
                copies.append(
                    weight_copy(t, part, lax.rem(t + 2 * q, tp), w_send.at[q, part])
                )
            copies.append(weight_copy(t, part, mate, w_send.at[0, part]))
        return copies

    for copy in own_weights():
        copy.start()

    win[t] = gated[span(t)]
    taps[t] = taps_ref[...]

    top_count = ids_ref.shape[1]
    spread_out = [
        jnp.broadcast_to(ids_ref[:, k : k + 1].astype(jnp.float32), (rows, rows))
        for k in range(top_count)
    ]
    across = [value.T for value in spread_out]
    down_place = lax.broadcasted_iota(jnp.int32, (rows, rows), 0)
    across_place = lax.broadcasted_iota(jnp.int32, (rows, rows), 1)
    table_ref[...] = jnp.zeros_like(table_ref)
    for k in range(top_count):
        count = jnp.zeros((1, rows), jnp.float32)
        for m in range(k + 1):
            same = spread_out[m] == across[k]
            if m == k:
                same = same & (down_place < across_place)
            count = count + jnp.sum(jnp.where(same, 1.0, 0.0), axis=0, keepdims=True)
        table_ref[pl.ds(k, 1)] = across[k][0:1] * room + count
        table_ref[pl.ds(top_count + k, 1)] = jnp.broadcast_to(
            share_ref[:, k : k + 1], (rows, rows)
        ).T[0:1]


    for p in range(1, tp):
        other = lax.rem(t + p, tp)
        pltpu.make_async_copy(win.at[other], win.at[other], win_recv.at[other]).wait()
        pltpu.make_async_copy(taps.at[other], taps.at[other], tap_recv.at[other]).wait()

    @pl.when((t == 0) & (z > 0))
    def _():
        for s in range(tp):
            pltpu.make_async_copy(low.at[s], low.at[s], halo_recv.at[1, s]).wait()
            win[s, pl.ds(0, edge)] = low[s]

    @pl.when((t == tp - 1) & (z < n - 1))
    def _():
        for s in range(tp):
            pltpu.make_async_copy(high.at[s], high.at[s], halo_recv.at[0, s]).wait()
            win[s, pl.ds(edge + rows, edge)] = high[s]

    def convolve(s, carry):
        first, second = carry
        wide[...] = win[s].astype(jnp.float32)
        tile = 64
        sums, squares = [], []
        for r in range(0, rows, tile):
            value = jnp.zeros((tile, chans), jnp.float32)
            for i in range(taps_count):
                value = value + taps[s, pl.ds(i, 1)] * wide[pl.ds(edge - half + i + r, tile)]
            mixed[s, pl.ds(r, tile)] = value
            sums.append(jnp.sum(value, axis=1, keepdims=True))
            squares.append(jnp.sum(value * value, axis=1, keepdims=True))
        return first + jnp.concatenate(sums, axis=0), second + jnp.concatenate(squares, axis=0)

    zero = jnp.zeros((rows, 1), jnp.float32)
    sums, squares = lax.fori_loop(0, tp, convolve, (zero, zero))
    center = sums / (chans * tp)
    spread = squares / (chans * tp) - center * center
    scale = lax.rsqrt(spread + 0.05)

    def activate(s, carry):
        value = (mixed[s] - center) * scale * taps[s, pl.ds(taps_count, 1)]
        act[s] = jax.nn.silu(value).astype(jnp.bfloat16)
        return carry

    lax.fori_loop(0, tp, activate, 0)

    def multiply(source):
        for c in range(0, width, 512):
            spot = pl.ds(c, 512)
            total[:, spot] += jnp.dot(
                act[source], weights[source, :, spot], preferred_element_type=jnp.float32
            )

    def landed(source):
        for part in range(2):
            spot = weights.at[source, pl.ds(part * halves, halves)]
            pltpu.make_async_copy(spot, spot, w_recv.at[source, part]).wait()

    loads[3].wait()
    total[...] = latent_ref[...].astype(jnp.float32)
    multiply(t)
    landed(mate)
    multiply(mate)

    def passing(q, part):
        source = lax.rem(t + 2 * q, tp)
        return weight_copy(source, part, mate, w_pass.at[q, part])

    for q in range(1, tp // 2):
        source = lax.rem(t + 2 * q, tp)
        for part in range(2):
            spot = weights.at[source, pl.ds(part * halves, halves)]
            pltpu.make_async_copy(spot, spot, w_recv.at[source, part]).wait()
            passing(q, part).start()
        multiply(source)
    for q in range(1, tp // 2):
        source = lax.rem(mate + 2 * q, tp)
        landed(source)
        multiply(source)

    for r in range(0, rows, 32):
        spot = pl.ds(r, 32)
        after = total[spot].astype(jnp.bfloat16)
        after_ref[spot] = after
        after = after.astype(jnp.float32)
        norm = lax.rsqrt(jnp.mean(after * after, axis=1, keepdims=True) + 0.01)
        in_ref[spot] = (after * norm * gain_ref[...]).astype(jnp.bfloat16)

    for p in range(1, tp):
        win_copy(p).wait_send()
        tap_copy(p).wait_send()
    for copy in own_weights():
        copy.wait_send()
    for q in range(1, tp // 2):
        for part in range(2):
            passing(q, part).wait_send()

    @pl.when(z < n - 1)
    def _():
        halo_copy(1).wait_send()

    @pl.when(z > 0)
    def _():
        halo_copy(0).wait_send()


def branch_and_norm(
    value, gate, conv_taps, conv_gain, point_weight, latents, channel_gain, ids, shares, room
):
    n, tp = lax.axis_size("sp"), lax.axis_size("tp")
    block, chans = value.shape
    rows, width = latents.shape
    taps_count = conv_taps.shape[0]
    edge = -(-(taps_count // 2) // 16) * 16
    table = jnp.concatenate([conv_taps, conv_gain[None, :]], axis=0)
    table = jnp.pad(table, ((0, -table.shape[0] % 8), (0, 0)))
    dma = pltpu.SemaphoreType.DMA
    bf16, f32 = jnp.bfloat16, jnp.float32
    anywhere = pl.BlockSpec(memory_space=pl.ANY)
    vmem = pl.BlockSpec(memory_space=pltpu.VMEM)
    return pl.pallas_call(
        functools.partial(branch_kernel, n, tp, taps_count, room),
        out_shape=[jax.ShapeDtypeStruct((rows, width), bf16)] * 2
        + [jax.ShapeDtypeStruct((8, rows), f32)],
        in_specs=[anywhere, anywhere, vmem, anywhere, anywhere, vmem, vmem, vmem],
        out_specs=[vmem] * 3,
        scratch_shapes=[
            pltpu.VMEM((block, chans), bf16),
            pltpu.VMEM((block, chans), bf16),
            pltpu.VMEM((rows, width), bf16),
            dma((4,)),
            pltpu.VMEM((block + 2 * edge, chans), bf16),
            pltpu.VMEM((tp, rows + 2 * edge, chans), bf16),
            pltpu.VMEM((tp, edge, chans), bf16),
            pltpu.VMEM((tp, edge, chans), bf16),
            pltpu.VMEM((tp,) + table.shape, f32),
            pltpu.VMEM((rows + 2 * edge, chans), f32),
            pltpu.VMEM((tp, rows, chans), f32),
            pltpu.VMEM((tp, rows, chans), bf16),
            pltpu.VMEM((tp, chans, width), bf16),
            pltpu.VMEM((rows, width), f32),
            dma((tp,)),
            dma((tp,)),
            dma((2,)),
            dma((2, tp)),
            dma((tp,)),
            dma((tp,)),
            dma((tp // 2, 2)),
            dma((tp // 2, 2)),
            dma((tp, 2)),
        ],
        compiler_params=pltpu.CompilerParams(
            collective_id=1, has_side_effects=True, vmem_limit_bytes=48 * 2**20
        ),
        name="branch",
    )(value, gate, table, point_weight, latents, channel_gain[None, :], ids, shares)


def shards(
    latents,
    conv_value,
    conv_gate,
    conv_taps,
    conv_gain,
    point_weight,
    channel_gain,
    expert_ids,
    expert_weights,
    gate_weight,
    up_weight,
    down_weight,
):
    row_count, top_count = expert_ids.shape
    experts = gate_weight.shape[0] * lax.axis_size(("sp", "tp"))
    capacity = 2 * top_count * row_count // experts
    room = -(-capacity // 16) * 16
    after, expert_in, table = branch_and_norm(
        conv_value, conv_gate, conv_taps, conv_gain, point_weight, latents, channel_gain,
        expert_ids, expert_weights, room,
    )
    return experts_and_back(
        expert_in, table, after, gate_weight, up_weight, down_weight, room
    )


def solution(mesh):
    return jax.shard_map(
        shards,
        mesh=mesh,
        in_specs=(
            P(("grp", "sp", "tp"), None),
            P(("grp", "sp"), "tp"),
            P(("grp", "sp"), "tp"),
            P(None, "tp"),
            P("tp"),
            P("tp", None),
            P(),
            P(("grp", "sp", "tp"), None),
            P(("grp", "sp", "tp"), None),
            P(("sp", "tp"), None, None),
            P(("sp", "tp"), None, None),
            P(("sp", "tp"), None, None),
        ),
        out_specs=P(("grp", "sp", "tp"), None),
        check_vma=False,
    )
```

```python
import functools

import jax
import jax.numpy as jnp
from jax import lax
from jax.experimental import pallas as pl
from jax.experimental.pallas import tpu as pltpu
from jax.sharding import PartitionSpec as P


MESH = pl.DeviceIdType.MESH
CHUNKS = 8


def expert_kernel(
    n, tp, cap, x_hbm, tab_hbm, after_ref, wg_hbm, wu_hbm, wd_hbm, out_ref,
    toks, tabs, comp, arr, back, inc, acc, wg, wu, wd, hid,
    own_sem, w_sem, tok_send, tok_recv, tab_send, tab_recv,
    piece_send, piece_recv, back_send, back_recv, sum_send, sum_recv,
):
    z = lax.axis_index("sp")
    t = lax.axis_index("tp")
    rows, width = after_ref.shape
    slots = tp * cap
    hidden_width = wg.shape[1]
    part_rows = rows // CHUNKS
    own_tok = pltpu.make_async_copy(x_hbm, toks.at[z], own_sem.at[0])
    own_tab = pltpu.make_async_copy(tab_hbm, tabs.at[z], own_sem.at[1])
    own_tok.start()
    own_tab.start()
    loads = [
        pltpu.make_async_copy(a, b, w_sem.at[i])
        for i, (a, b) in enumerate(((wg_hbm.at[0], wg), (wu_hbm.at[0], wu), (wd_hbm.at[0], wd)))
    ]
    for load in loads:
        load.start()

    barrier = pltpu.get_barrier_semaphore()
    for p in range(1, tp):
        pl.semaphore_signal(
            barrier, inc=1, device_id={"tp": lax.rem(t + p, tp)}, device_id_type=MESH
        )

    @pl.when(z > 0)
    def _():
        pl.semaphore_signal(barrier, inc=1, device_id={"sp": z - 1}, device_id_type=MESH)

    @pl.when(z < n - 1)
    def _():
        pl.semaphore_signal(barrier, inc=1, device_id={"sp": z + 1}, device_id_type=MESH)

    peers = tp - 1 + (z > 0).astype(jnp.int32) + (z < n - 1).astype(jnp.int32)
    pl.semaphore_wait(barrier, peers)

    own_tok.wait()
    own_tab.wait()

    def source(j):
        low = jnp.minimum(z, n - 1 - z)
        near = jnp.where(j % 2 == 1, z - (j + 1) // 2, z + j // 2)
        far = jnp.where(z > n - 1 - z, z - (j - low), z + (j - low))
        return jnp.where(j <= 2 * low, near, far)

    def token_copies(zs, side):
        target = z + 1 if side else z - 1
        return [
            pltpu.make_async_remote_copy(
                src_ref=ref.at[zs],
                dst_ref=ref.at[zs],
                send_sem=ss.at[side, zs],
                recv_sem=rs.at[zs],
                device_id={"sp": target},
                device_id_type=MESH,
            )
            for ref, ss, rs in ((tabs, tab_send, tab_recv), (toks, tok_send, tok_recv))
        ]

    def span(index):
        return pl.ds(pl.multiple_of(index * cap, 16), cap)

    def exchange(j, to_ref, zs, ss, rs):
        page = lax.rem(j, 2)
        for p in range(1, tp):
            other = lax.rem(t + p, tp)
            pltpu.make_async_remote_copy(
                src_ref=comp.at[page, span(other)],
                dst_ref=to_ref.at[zs, span(t)],
                send_sem=ss.at[zs],
                recv_sem=rs.at[zs],
                device_id={"tp": other},
                device_id_type=MESH,
            ).start()
        to_ref[zs, span(t)] = comp[page, span(t)]

    def wait_pieces(ref, zs, ss, rs):
        part = ref.at[zs, pl.ds(0, (tp - 1) * cap)]
        pltpu.make_async_copy(part, part, rs.at[zs]).wait()
        pltpu.make_async_copy(part, part, ss.at[zs]).wait()

    def sum_copy(zs, k, side):
        target = z + 1 if side else z - 1
        slot = jnp.where(target == zs, n, zs) if side else zs
        piece = pl.ds(k * part_rows, part_rows)
        return pltpu.make_async_remote_copy(
            src_ref=toks.at[zs, piece],
            dst_ref=inc.at[slot, piece],
            send_sem=sum_send.at[zs, k],
            recv_sem=sum_recv.at[slot, k],
            device_id={"sp": target},
            device_id_type=MESH,
        )

    def names(zs):
        table = tabs[zs]
        base = (z * slots).astype(jnp.float32)
        place = lax.broadcasted_iota(jnp.int32, (slots, rows), 0).astype(jnp.float32) + base
        return place == table[0:1, :], place == table[1:2, :], table

    def passes_on(zs):
        return ((zs <= z) & (z < n - 1)) | ((zs >= z) & (z > 0))

    def arrive(zs):
        pltpu.make_async_copy(tabs.at[zs], tabs.at[zs], tab_recv.at[zs]).wait()
        pltpu.make_async_copy(toks.at[zs], toks.at[zs], tok_recv.at[zs]).wait()

    def forward(zs):
        @pl.when((zs <= z) & (z < n - 1))
        def _():
            for copy in token_copies(zs, 1):
                copy.start()

        @pl.when((zs >= z) & (z > 0))
        def _():
            for copy in token_copies(zs, 0):
                copy.start()

    def hand_on(j):
        zs = source(j)

        @pl.when((j < n) & passes_on(zs))
        def _():
            arrive(zs)
            forward(zs)

    def take(j):
        zs = source(j)

        @pl.when((j > 0) & jnp.logical_not(passes_on(zs)))
        def _():
            arrive(zs)

        first, second, _ = names(zs)
        pick = jnp.where(first | second, 1.0, 0.0).astype(jnp.bfloat16)
        comp[lax.rem(j, 2)] = jnp.dot(pick, toks[zs], preferred_element_type=jnp.float32).astype(jnp.bfloat16)
        exchange(j, arr, zs, piece_send, piece_recv)

    def run(j):
        zs = source(j)

        @pl.when(j == 0)
        def _():
            for load in loads:
                load.wait()

        wait_pieces(arr, zs, piece_send, piece_recv)
        step = 256
        for f in range(0, hidden_width, step):
            gate = jnp.dot(arr[zs], wg[:, f : f + step], preferred_element_type=jnp.float32)
            up = jnp.dot(arr[zs], wu[:, f : f + step], preferred_element_type=jnp.float32)
            hid[:, f : f + step] = (jax.nn.silu(gate) * up).astype(jnp.bfloat16)
        step = 512
        for c in range(0, width, step):
            comp[lax.rem(j, 2), :, c : c + step] = jnp.dot(
                hid[...], wd[:, c : c + step], preferred_element_type=jnp.float32
            ).astype(jnp.bfloat16)
        exchange(j, back, zs, back_send, back_recv)

    def merge(j):
        zs = source(j)
        wait_pieces(back, zs, back_send, back_recv)
        first, second, table = names(zs)
        share = jnp.where(first, table[2:3, :], 0.0) + jnp.where(second, table[3:4, :], 0.0)
        share = share.T
        high = share.astype(jnp.bfloat16)
        rest = (share - high.astype(jnp.float32)).astype(jnp.bfloat16)

        def total():
            return jnp.dot(high, back[zs], preferred_element_type=jnp.float32) + jnp.dot(
                rest, back[zs], preferred_element_type=jnp.float32
            )

        @pl.when((zs <= z) & (z < n - 1))
        def _():
            for copy in token_copies(zs, 1):
                copy.wait_send()

        @pl.when((zs >= z) & (z > 0))
        def _():
            for copy in token_copies(zs, 0):
                copy.wait_send()

        value = total()

        @pl.when(zs == z)
        def _():
            acc[...] = value

        @pl.when(zs != z)
        def _():
            toks[zs] = value.astype(jnp.bfloat16)

        @pl.when((zs < z) & (z == n - 1))
        def _():
            for k in range(CHUNKS):
                sum_copy(zs, k, 0).start()

        @pl.when((zs > z) & (z == 0))
        def _():
            for k in range(CHUNKS):
                sum_copy(zs, k, 1).start()

    forward(z)

    def body(j, carry):
        @pl.when(j > 0)
        def _():
            run(j - 1)

        @pl.when(j == 1)
        def _():
            hand_on(j)

        @pl.when(j > 0)
        def _():
            hand_on(j + 1)

        @pl.when(j < n)
        def _():
            take(j)

        @pl.when(j > 0)
        def _():
            merge(j - 1)

        return carry

    lax.fori_loop(0, n + 1, body, 0)

    def relay(side):
        def one(d, carry):
            zs = z + d if side else z - d

            @pl.when((zs <= n - 1) if side else (zs >= 0))
            def _():
                for k in range(CHUNKS):
                    piece = pl.ds(k * part_rows, part_rows)
                    spot = inc.at[zs, piece]
                    pltpu.make_async_copy(spot, spot, sum_recv.at[zs, k]).wait()
                    toks[zs, piece] = (
                        toks[zs, piece].astype(jnp.float32) + inc[zs, piece].astype(jnp.float32)
                    ).astype(jnp.bfloat16)
                    sum_copy(zs, k, side).start()

            return carry

        lax.fori_loop(1, n - 1, one, 0)

    upper = z > n - 1 - z

    @pl.when(upper & (z < n - 1))
    def _():
        relay(0)

    @pl.when(z > 0)
    def _():
        relay(1)

    @pl.when((z <= n - 1 - z) & (z < n - 1))
    def _():
        relay(0)

    for k in range(CHUNKS):
        piece = pl.ds(k * part_rows, part_rows)

        @pl.when(z < n - 1)
        def _():
            spot = inc.at[z, piece]
            pltpu.make_async_copy(spot, spot, sum_recv.at[z, k]).wait()
            acc[piece] = acc[piece] + inc[z, piece].astype(jnp.float32)

        @pl.when(z > 0)
        def _():
            spot = inc.at[n, piece]
            pltpu.make_async_copy(spot, spot, sum_recv.at[n, k]).wait()
            acc[piece] = acc[piece] + inc[n, piece].astype(jnp.float32)

        out_ref[piece] = (after_ref[piece].astype(jnp.float32) + acc[piece]).astype(jnp.bfloat16)

    def drain(zs, carry):
        @pl.when(zs != z)
        def _():
            for k in range(CHUNKS):
                spot = toks.at[zs, pl.ds(k * part_rows, part_rows)]
                pltpu.make_async_copy(spot, spot, sum_send.at[zs, k]).wait()

        return carry

    lax.fori_loop(0, n, drain, 0)


def experts_and_back(expert_in, table, after, gate_weight, up_weight, down_weight, cap):
    n, tp = lax.axis_size("sp"), lax.axis_size("tp")
    rows, width = expert_in.shape
    hidden_width = gate_weight.shape[2]
    slots = tp * cap
    dma = pltpu.SemaphoreType.DMA
    bf16, f32 = jnp.bfloat16, jnp.float32
    anywhere = pl.BlockSpec(memory_space=pl.ANY)
    vmem = pl.BlockSpec(memory_space=pltpu.VMEM)
    return pl.pallas_call(
        functools.partial(expert_kernel, n, tp, cap),
        out_shape=jax.ShapeDtypeStruct((rows, width), bf16),
        in_specs=[anywhere, anywhere, vmem, anywhere, anywhere, anywhere],
        out_specs=vmem,
        scratch_shapes=[
            pltpu.VMEM((n, rows, width), bf16),
            pltpu.VMEM((n,) + table.shape, f32),
            pltpu.VMEM((2, slots, width), bf16),
            pltpu.VMEM((n, slots, width), bf16),
            pltpu.VMEM((n, slots, width), bf16),
            pltpu.VMEM((n + 1, rows, width), bf16),
            pltpu.VMEM((rows, width), f32),
            pltpu.VMEM((width, hidden_width), bf16),
            pltpu.VMEM((width, hidden_width), bf16),
            pltpu.VMEM((hidden_width, width), bf16),
            pltpu.VMEM((slots, hidden_width), bf16),
            dma((2,)),
            dma((3,)),
            dma((2, n)),
            dma((n,)),
            dma((2, n)),
            dma((n,)),
            dma((n,)),
            dma((n,)),
            dma((n,)),
            dma((n,)),
            dma((n, CHUNKS)),
            dma((n + 1, CHUNKS)),
        ],
        compiler_params=pltpu.CompilerParams(
            collective_id=0, has_side_effects=True, vmem_limit_bytes=67043328
        ),
        name="experts",
    )(expert_in, table, after, gate_weight, up_weight, down_weight)


def branch_kernel(
    n, tp, taps_count, room, value_hbm, gate_hbm, taps_ref, weight_hbm, latent_hbm, gain_ref,
    ids_ref, share_ref, after_ref, in_ref, table_ref,
    value_ref, gate_ref, latent_ref, load_sem, gated, win, low, high, taps, wide, mixed, act, weights, total,
    win_send, win_recv, halo_send, halo_recv, tap_send, tap_recv, w_send, w_pass, w_recv,
):
    z = lax.axis_index("sp")
    t = lax.axis_index("tp")
    block, chans = value_ref.shape
    rows, width = latent_ref.shape
    edge = low.shape[1]
    half = taps_count // 2
    view = rows + 2 * edge
    mate = t + 1 - 2 * lax.rem(t, 2)
    halves = chans // 2
    loads = [
        pltpu.make_async_copy(a, b, load_sem.at[i])
        for i, (a, b) in enumerate(
            (
                (value_hbm, value_ref),
                (gate_hbm, gate_ref),
                (weight_hbm, weights.at[t]),
                (latent_hbm, latent_ref),
            )
        )
    ]
    for load in loads:
        load.start()

    barrier = pltpu.get_barrier_semaphore()
    for p in range(tp):
        other = lax.rem(t + p, tp)
        if p:
            pl.semaphore_signal(barrier, inc=1, device_id={"tp": other}, device_id_type=MESH)

        @pl.when(z > 0)
        def _():
            pl.semaphore_signal(
                barrier, inc=1, device_id={"sp": z - 1, "tp": other}, device_id_type=MESH
            )

        @pl.when(z < n - 1)
        def _():
            pl.semaphore_signal(
                barrier, inc=1, device_id={"sp": z + 1, "tp": other}, device_id_type=MESH
            )

    gated[pl.ds(0, edge)] = jnp.zeros((edge, chans), jnp.bfloat16)
    gated[pl.ds(edge + block, edge)] = jnp.zeros((edge, chans), jnp.bfloat16)
    loads[0].wait()
    loads[1].wait()
    step = 64
    for r in range(0, block, step):
        value = value_ref[pl.ds(r, step)].astype(jnp.float32)
        gate = gate_ref[pl.ds(r, step)].astype(jnp.float32)
        gated[pl.ds(edge + r, step)] = (value * jax.nn.sigmoid(gate)).astype(jnp.bfloat16)

    peers = tp - 1 + tp * ((z > 0).astype(jnp.int32) + (z < n - 1).astype(jnp.int32))
    pl.semaphore_wait(barrier, peers)

    def span(index):
        return pl.ds(pl.multiple_of(index * rows, 16), view)

    def win_copy(p):
        other = lax.rem(t + p, tp)
        return pltpu.make_async_remote_copy(
            src_ref=gated.at[span(other)], dst_ref=win.at[t],
            send_sem=win_send.at[p], recv_sem=win_recv.at[t],
            device_id={"tp": other}, device_id_type=MESH,
        )

    def tap_copy(p):
        other = lax.rem(t + p, tp)
        return pltpu.make_async_remote_copy(
            src_ref=taps_ref, dst_ref=taps.at[t],
            send_sem=tap_send.at[p], recv_sem=tap_recv.at[t],
            device_id={"tp": other}, device_id_type=MESH,
        )

    def halo_copy(up):
        start = block if up else edge
        place = low if up else high
        return pltpu.make_async_remote_copy(
            src_ref=gated.at[pl.ds(start, edge)], dst_ref=place.at[t],
            send_sem=halo_send.at[up], recv_sem=halo_recv.at[up, t],
            device_id={"sp": z + 1 if up else z - 1, "tp": jnp.int32(0 if up else tp - 1)},
            device_id_type=MESH,
        )

    @pl.when(z < n - 1)
    def _():
        halo_copy(1).start()

    @pl.when(z > 0)
    def _():
        halo_copy(0).start()

    for p in range(1, tp):
        win_copy(p).start()
        tap_copy(p).start()

    loads[2].wait()

    def weight_copy(source, part, target, send_sem):
        spot = pl.ds(part * halves, halves)
        return pltpu.make_async_remote_copy(
            src_ref=weights.at[source, spot],
            dst_ref=weights.at[source, spot],
            send_sem=send_sem, recv_sem=w_recv.at[source, part],
            device_id={"tp": target}, device_id_type=MESH,
        )

    def own_weights():
        copies = []
        for part in range(2):
            for q in range(1, tp // 2):
                copies.append(
                    weight_copy(t, part, lax.rem(t + 2 * q, tp), w_send.at[q, part])
                )
            copies.append(weight_copy(t, part, mate, w_send.at[0, part]))
        return copies

    for copy in own_weights():
        copy.start()

    win[t] = gated[span(t)]
    taps[t] = taps_ref[...]

    top_count = ids_ref.shape[1]
    spread_out = [
        jnp.broadcast_to(ids_ref[:, k : k + 1].astype(jnp.float32), (rows, rows))
        for k in range(top_count)
    ]
    across = [value.T for value in spread_out]
    down_place = lax.broadcasted_iota(jnp.int32, (rows, rows), 0)
    across_place = lax.broadcasted_iota(jnp.int32, (rows, rows), 1)
    table_ref[...] = jnp.zeros_like(table_ref)
    for k in range(top_count):
        count = jnp.zeros((1, rows), jnp.float32)
        for m in range(k + 1):
            same = spread_out[m] == across[k]
            if m == k:
                same = same & (down_place < across_place)
            count = count + jnp.sum(jnp.where(same, 1.0, 0.0), axis=0, keepdims=True)
        table_ref[pl.ds(k, 1)] = across[k][0:1] * room + count
        table_ref[pl.ds(top_count + k, 1)] = jnp.broadcast_to(
            share_ref[:, k : k + 1], (rows, rows)
        ).T[0:1]


    for p in range(1, tp):
        other = lax.rem(t + p, tp)
        pltpu.make_async_copy(win.at[other], win.at[other], win_recv.at[other]).wait()
        pltpu.make_async_copy(taps.at[other], taps.at[other], tap_recv.at[other]).wait()

    @pl.when((t == 0) & (z > 0))
    def _():
        for s in range(tp):
            pltpu.make_async_copy(low.at[s], low.at[s], halo_recv.at[1, s]).wait()
            win[s, pl.ds(0, edge)] = low[s]

    @pl.when((t == tp - 1) & (z < n - 1))
    def _():
        for s in range(tp):
            pltpu.make_async_copy(high.at[s], high.at[s], halo_recv.at[0, s]).wait()
            win[s, pl.ds(edge + rows, edge)] = high[s]

    def convolve(s, carry):
        first, second = carry
        wide[...] = win[s].astype(jnp.float32)
        tile = 64
        sums, squares = [], []
        for r in range(0, rows, tile):
            value = jnp.zeros((tile, chans), jnp.float32)
            for i in range(taps_count):
                value = value + taps[s, pl.ds(i, 1)] * wide[pl.ds(edge - half + i + r, tile)]
            mixed[s, pl.ds(r, tile)] = value
            sums.append(jnp.sum(value, axis=1, keepdims=True))
            squares.append(jnp.sum(value * value, axis=1, keepdims=True))
        return first + jnp.concatenate(sums, axis=0), second + jnp.concatenate(squares, axis=0)

    zero = jnp.zeros((rows, 1), jnp.float32)
    sums, squares = lax.fori_loop(0, tp, convolve, (zero, zero))
    center = sums / (chans * tp)
    spread = squares / (chans * tp) - center * center
    scale = lax.rsqrt(spread + 0.05)

    def activate(s, carry):
        value = (mixed[s] - center) * scale * taps[s, pl.ds(taps_count, 1)]
        act[s] = jax.nn.silu(value).astype(jnp.bfloat16)
        return carry

    lax.fori_loop(0, tp, activate, 0)

    def multiply(source):
        for c in range(0, width, 512):
            spot = pl.ds(c, 512)
            total[:, spot] += jnp.dot(
                act[source], weights[source, :, spot], preferred_element_type=jnp.float32
            )

    def landed(source):
        for part in range(2):
            spot = weights.at[source, pl.ds(part * halves, halves)]
            pltpu.make_async_copy(spot, spot, w_recv.at[source, part]).wait()

    loads[3].wait()
    total[...] = latent_ref[...].astype(jnp.float32)
    multiply(t)
    landed(mate)
    multiply(mate)

    def passing(q, part):
        source = lax.rem(t + 2 * q, tp)
        return weight_copy(source, part, mate, w_pass.at[q, part])

    for q in range(1, tp // 2):
        source = lax.rem(t + 2 * q, tp)
        for part in range(2):
            spot = weights.at[source, pl.ds(part * halves, halves)]
            pltpu.make_async_copy(spot, spot, w_recv.at[source, part]).wait()
            passing(q, part).start()
        multiply(source)
    for q in range(1, tp // 2):
        source = lax.rem(mate + 2 * q, tp)
        landed(source)
        multiply(source)

    for r in range(0, rows, 32):
        spot = pl.ds(r, 32)
        after = total[spot].astype(jnp.bfloat16)
        after_ref[spot] = after
        after = after.astype(jnp.float32)
        norm = lax.rsqrt(jnp.mean(after * after, axis=1, keepdims=True) + 0.01)
        in_ref[spot] = (after * norm * gain_ref[...]).astype(jnp.bfloat16)

    for p in range(1, tp):
        win_copy(p).wait_send()
        tap_copy(p).wait_send()
    for copy in own_weights():
        copy.wait_send()
    for q in range(1, tp // 2):
        for part in range(2):
            passing(q, part).wait_send()

    @pl.when(z < n - 1)
    def _():
        halo_copy(1).wait_send()

    @pl.when(z > 0)
    def _():
        halo_copy(0).wait_send()


def branch_and_norm(
    value, gate, conv_taps, conv_gain, point_weight, latents, channel_gain, ids, shares, room
):
    n, tp = lax.axis_size("sp"), lax.axis_size("tp")
    block, chans = value.shape
    rows, width = latents.shape
    taps_count = conv_taps.shape[0]
    edge = -(-(taps_count // 2) // 16) * 16
    table = jnp.concatenate([conv_taps, conv_gain[None, :]], axis=0)
    table = jnp.pad(table, ((0, -table.shape[0] % 8), (0, 0)))
    dma = pltpu.SemaphoreType.DMA
    bf16, f32 = jnp.bfloat16, jnp.float32
    anywhere = pl.BlockSpec(memory_space=pl.ANY)
    vmem = pl.BlockSpec(memory_space=pltpu.VMEM)
    return pl.pallas_call(
        functools.partial(branch_kernel, n, tp, taps_count, room),
        out_shape=[jax.ShapeDtypeStruct((rows, width), bf16)] * 2
        + [jax.ShapeDtypeStruct((8, rows), f32)],
        in_specs=[anywhere, anywhere, vmem, anywhere, anywhere, vmem, vmem, vmem],
        out_specs=[vmem] * 3,
        scratch_shapes=[
            pltpu.VMEM((block, chans), bf16),
            pltpu.VMEM((block, chans), bf16),
            pltpu.VMEM((rows, width), bf16),
            dma((4,)),
            pltpu.VMEM((block + 2 * edge, chans), bf16),
            pltpu.VMEM((tp, rows + 2 * edge, chans), bf16),
            pltpu.VMEM((tp, edge, chans), bf16),
            pltpu.VMEM((tp, edge, chans), bf16),
            pltpu.VMEM((tp,) + table.shape, f32),
            pltpu.VMEM((rows + 2 * edge, chans), f32),
            pltpu.VMEM((tp, rows, chans), f32),
            pltpu.VMEM((tp, rows, chans), bf16),
            pltpu.VMEM((tp, chans, width), bf16),
            pltpu.VMEM((rows, width), f32),
            dma((tp,)),
            dma((tp,)),
            dma((2,)),
            dma((2, tp)),
            dma((tp,)),
            dma((tp,)),
            dma((tp // 2, 2)),
            dma((tp // 2, 2)),
            dma((tp, 2)),
        ],
        compiler_params=pltpu.CompilerParams(
            collective_id=1, has_side_effects=True, vmem_limit_bytes=67043328
        ),
        name="branch",
    )(value, gate, table, point_weight, latents, channel_gain[None, :], ids, shares)


def shards(
    latents,
    conv_value,
    conv_gate,
    conv_taps,
    conv_gain,
    point_weight,
    channel_gain,
    expert_ids,
    expert_weights,
    gate_weight,
    up_weight,
    down_weight,
):
    row_count, top_count = expert_ids.shape
    experts = gate_weight.shape[0] * lax.axis_size(("sp", "tp"))
    capacity = 2 * top_count * row_count // experts
    room = -(-capacity // 16) * 16
    after, expert_in, table = branch_and_norm(
        conv_value, conv_gate, conv_taps, conv_gain, point_weight, latents, channel_gain,
        expert_ids, expert_weights, room,
    )
    return experts_and_back(
        expert_in, table, after, gate_weight, up_weight, down_weight, room
    )


def solution(mesh):
    return jax.shard_map(
        shards,
        mesh=mesh,
        in_specs=(
            P(("grp", "sp", "tp"), None),
            P(("grp", "sp"), "tp"),
            P(("grp", "sp"), "tp"),
            P(None, "tp"),
            P("tp"),
            P("tp", None),
            P(),
            P(("grp", "sp", "tp"), None),
            P(("grp", "sp", "tp"), None),
            P(("sp", "tp"), None, None),
            P(("sp", "tp"), None, None),
            P(("sp", "tp"), None, None),
        ),
        out_specs=P(("grp", "sp", "tp"), None),
        check_vma=False,
    )
```
